256 devices in a mesh: sp: 64 (over z, y, core), tp: 4 (over x).
Axes of the slice: x: 4, y: 4, z: 8, core: 2. Of those that a mesh axis runs over, the one named last changes fastest.
Arguments:
- queries: bfloat16 [16384, 2048], P('sp', 'tp'), may hold values from -6 to 6
- keys: bfloat16 [16384, 512], P('sp', 'tp'), may hold values from -6 to 6
- values: bfloat16 [16384, 512], P('sp', 'tp'), may hold values from -6 to 6
- query_gain: float32 [64], replicated, may hold values from 0.8 to 5
- key_gain: float32 [64], replicated, may hold values from 0.8 to 5
- stream: bfloat16 [16384, 2048], P('sp'), may hold values from -0.1796875 to 0.1796875
- out_weight: bfloat16 [2048, 2048], P('tp'), may hold values from -0.125 to 0.125
- mixer_gain: float32 [2048], replicated, may hold values from 0.1 to 1.9
- up_weight: bfloat16 [2048, 8192], P('sp', 'tp'), may hold values from -0.125 to 0.125
- down_weight: bfloat16 [8192, 2048], P('tp', 'sp'), may hold values from -0.0625 to 0.0625
Outputs:
- updated: bfloat16 [16384, 2048], P('sp', 'tp')
The draws below stay inside these ranges and needn't reach their ends.
All inputs are finite; a program needn't handle non-finite values.
Results may differ from the reference program's by a relative error of at most 0.02.
The reference program's roundings to bfloat16 on the way count: a program that leaves them out, or rounds other values in their place, can miss the bound.
Values may be sent and summed in bfloat16 or wider, within the bound.
A program may use at most 128 MiB of HBM per device.

```python
import math
import jax
import jax.numpy as jnp
from jax import lax

D = 2048
HQ = 32
KVH = 8
HD = 64
FF = 8192
GRID_W = 64
TOKENS = 16384
N_TP = 4


def drawn(key):
    query_key = jax.random.fold_in(key, 101)
    key_key = jax.random.fold_in(key, 202)
    key_draw = jax.random.normal(key_key, (TOKENS, KVH * HD), jnp.float32)
    query_draw = jax.random.normal(query_key, (TOKENS, HQ * HD), jnp.float32)
    return (jnp.clip(query_draw, -6.0, 6.0), jnp.clip(key_draw, -6.0, 6.0))


def draw_queries(key, part):
    return drawn(key)[0].astype(jnp.bfloat16)


def draw_keys(key, part):
    return drawn(key)[1].astype(jnp.bfloat16)


def gain_draw(key, salt):
    gain_key = jax.random.fold_in(key, salt)
    return jax.random.uniform(gain_key, (HD,), jnp.float32, 0.8, 1.8)


def draw_query_gain(key, part):
    return gain_draw(key, 303)


def draw_key_gain(key, part):
    return gain_draw(key, 404)


def shard_levels(key, extent, pieces, low, high):
    gain, own = 1.0, jax.random.fold_in(key, 6)
    for dim, shards_of in pieces:
        heights = jnp.exp(jax.random.uniform(jax.random.fold_in(own, dim), (shards_of,), jnp.float32, low / len(pieces), high / len(pieces)))
        gain = gain * jnp.repeat(heights, extent[dim] // shards_of).reshape([-1 if axis == dim else 1 for axis in range(len(extent))])
    return gain


def bell_draw(stream_key, shape, spread, limit, cuts=(), held_as=jnp.bfloat16):
    loudness = shard_levels(stream_key, shape, cuts, -0.22, 0.18) if cuts else 1.0
    array = jax.random.normal(stream_key, shape, jnp.float32) * spread * loudness
    return jnp.minimum(jnp.maximum(array, -limit), limit).astype(held_as)


def setup_inputs(seed: int = 0) -> dict:
    seeds = jax.random.split(jax.random.key(seed), 11)
    queries = draw_queries(jax.random.fold_in(seeds[10], 71), 0)
    keys = draw_keys(jax.random.fold_in(seeds[10], 71), 0)
    values = bell_draw(seeds[2], (TOKENS, KVH * HD), 1.0, 6.0, ((0, 64), (1, 4)))
    query_gain = draw_query_gain(jax.random.fold_in(seeds[10], 71), 0)
    key_gain = draw_key_gain(jax.random.fold_in(seeds[10], 71), 0)
    stream = bell_draw(seeds[5], (TOKENS, D), 0.03, 0.1796875, ((0, 64),))
    out_weight = bell_draw(seeds[6], (HQ * HD, D), (HQ * HD) ** -0.5, 0.125, ((0, 4),))
    mixer_gain = jnp.clip(1.0 + 0.18 * jax.random.normal(seeds[7], (D,), jnp.float32), 0.1, 1.9)
    up_weight = bell_draw(seeds[8], (D, FF), D ** -0.5, 0.125, ((0, 64), (1, 4)))
    down_weight = bell_draw(seeds[9], (FF, D), FF ** -0.5, 0.0625, ((0, 4), (1, 64)))
    return dict(queries=queries, keys=keys, values=values, query_gain=query_gain, key_gain=key_gain, stream=stream, out_weight=out_weight, mixer_gain=mixer_gain, up_weight=up_weight, down_weight=down_weight)


EPSILON = 1e-06

def prepare(projected, gain_vec, offset):
    row_count = projected.shape[0]
    head_count = projected.shape[1] // HD
    widened = projected.astype(jnp.float32).reshape(row_count, head_count, HD)
    widened = widened * lax.rsqrt(lax.optimization_barrier(jnp.mean(widened * widened, axis=-1, keepdims=True)) + EPSILON) * gain_vec
    position = offset + jnp.arange(row_count, dtype=jnp.int32)
    grid_row = (position // GRID_W).astype(jnp.float32)
    grid_col = (position % GRID_W).astype(jnp.float32)
    half_dim = HD // 2
    inverse = 1.0 / jnp.power(10000.0, jnp.arange(0, half_dim, 2, dtype=jnp.float32) / half_dim)
    angle = jnp.concatenate([grid_row[:, None] * inverse, grid_col[:, None] * inverse], axis=-1)
    cosine = jnp.cos(angle)[:, None, :]
    sine_table = jnp.sin(angle)[:, None, :]
    paired = widened.reshape(row_count, head_count, half_dim, 2)
    former = paired[..., 0]
    latter = paired[..., 1]
    rotated = jnp.stack([former * cosine - latter * sine_table, former * sine_table + latter * cosine], axis=-1)
    return rotated.reshape(row_count, head_count, HD).astype(jnp.bfloat16)

def grouped_sum(left, right, groups):
    width = left.shape[1] // groups
    total = jnp.zeros((left.shape[0], right.shape[1]), jnp.float32)
    for group_index in range(groups):
        term = jnp.dot(left[:, group_index * width:(group_index + 1) * width], right[group_index * width:(group_index + 1) * width], preferred_element_type=jnp.float32).astype(jnp.bfloat16)
        term = lax.optimization_barrier(term)
        total = total + term.astype(jnp.float32)
    return total

def reference(queries, keys, values, query_gain, key_gain, stream, out_weight, mixer_gain, up_weight, down_weight):
    group_size = HQ // KVH
    prepared_queries = prepare(queries, query_gain, 0)
    prepared_keys = prepare(keys, key_gain, 0)
    key_wide = prepared_keys.astype(jnp.float32)
    value_wide = values.reshape(TOKENS, KVH, HD).astype(jnp.float32)
    block_rows = math.gcd(TOKENS, 128)
    blocks = prepared_queries.reshape(TOKENS // block_rows, block_rows, KVH, group_size, HD)
    score_scale = 1.0 / math.sqrt(HD)

    def attend_rows(query_block):
        scores = jnp.einsum('qhgd,khd->hgqk', query_block.astype(jnp.float32), key_wide) * score_scale
        peak = lax.optimization_barrier(jnp.max(scores, axis=-1, keepdims=True))
        exps = jnp.exp(scores - peak)
        totals = lax.optimization_barrier(jnp.sum(exps, axis=-1))
        rounded = exps.astype(jnp.bfloat16)
        mixed = jnp.einsum('hgqk,khd->hgqd', rounded.astype(jnp.float32), value_wide)
        mixed = mixed / totals[..., None]
        return jnp.transpose(mixed, (2, 0, 1, 3)).reshape(block_rows, HQ * HD).astype(jnp.bfloat16)
    head_out = lax.map(attend_rows, blocks).reshape(TOKENS, HQ * HD)
    attended = grouped_sum(head_out, out_weight, N_TP)
    mid = (stream.astype(jnp.float32) + attended).astype(jnp.bfloat16)
    mid_wide = mid.astype(jnp.float32)
    normed = mid_wide * lax.rsqrt(lax.optimization_barrier(jnp.mean(mid_wide * mid_wide, axis=-1, keepdims=True)) + EPSILON) * mixer_gain
    normed = normed.astype(jnp.bfloat16)
    up_sums = jnp.dot(normed, up_weight, preferred_element_type=jnp.float32)
    hidden = jnp.square(jax.nn.relu(up_sums)).astype(jnp.bfloat16)
    down_sums = grouped_sum(hidden, down_weight, N_TP)
    return (mid_wide + down_sums).astype(jnp.bfloat16)
```

```python
import functools
import math

import jax
import jax.numpy as jnp
from jax import lax
from jax.experimental import pallas as pl
from jax.experimental.pallas import tpu as pltpu
from jax.sharding import PartitionSpec as P

HD = 64
GRID_W = 64
EPSILON = 1e-06
NZ, NY, NC = 8, 4, 2
SCALE = math.log2(math.e) / math.sqrt(HD)
MESH = pl.DeviceIdType.MESH
ORDER = (0, 1, 7, 2, 6, 3, 5, 4)


def prepare(projected, gain_vec, offset):
    row_count = projected.shape[0]
    head_count = projected.shape[1] // HD
    widened = projected.astype(jnp.float32).reshape(row_count, head_count, HD)
    widened = (
        widened
        * lax.rsqrt(jnp.mean(widened * widened, axis=-1, keepdims=True) + EPSILON)
        * gain_vec
    )
    position = offset + jnp.arange(row_count, dtype=jnp.int32)
    grid_row = (position // GRID_W).astype(jnp.float32)
    grid_col = (position % GRID_W).astype(jnp.float32)
    half_dim = HD // 2
    inverse = 1.0 / jnp.power(10000.0, jnp.arange(0, half_dim, 2, dtype=jnp.float32) / half_dim)
    angle = jnp.concatenate([grid_row[:, None] * inverse, grid_col[:, None] * inverse], axis=-1)
    cosine = jnp.cos(angle)[:, None, :]
    sine_table = jnp.sin(angle)[:, None, :]
    paired = widened.reshape(row_count, head_count, half_dim, 2)
    former = paired[..., 0]
    latter = paired[..., 1]
    rotated = jnp.stack(
        [former * cosine - latter * sine_table, former * sine_table + latter * cosine], axis=-1
    )
    return rotated.reshape(row_count, head_count, HD).astype(jnp.bfloat16)


class Place:
    def __init__(self):
        me = lax.axis_index("sp")
        self.me = me
        self.core = lax.rem(me, NC)
        self.y = lax.rem(me // NC, NY)
        self.z = me // (NC * NY)

    def zat(self, d):
        return lax.rem(self.z + (d + NZ) % NZ, NZ)

    def yat(self, d):
        return lax.rem(self.y + (d + NY) % NY, NY)

    def dev(self, dz=0, dy=0, other=False):
        core = 1 - self.core if other else self.core
        return (self.zat(dz) * NY + self.yat(dy)) * NC + core


class Mail:
    def __init__(self, place, send_sems, recv_sems):
        self.at, self.ss, self.rs, self.sent = place, send_sems, recv_sems, []

    def copy(self, key, ref, target):
        return pltpu.make_async_remote_copy(
            src_ref=ref,
            dst_ref=ref,
            send_sem=self.ss.at[key],
            recv_sem=self.rs.at[key],
            device_id={"sp": target},
            device_id_type=MESH,
        )

    def send(self, key, ref, target):
        self.copy(key, ref(), target()).start()
        self.sent.append((key, ref, target))

    def got(self, key, ref):
        self.copy(key, ref, self.at.dev(0, 1)).wait_recv()

    def finish(self):
        for key, ref, target in self.sent:
            self.copy(key, ref(), target()).wait_send()


class ZFirst(Mail):
    SEMS = 48

    def __init__(self, buf, half, *rest):
        super().__init__(*rest)
        self.buf, self.half = buf, half

    def slot(self, r, dy=0):
        return self.buf.at[self.at.zat(r), self.at.yat(dy), self.at.core]

    def part(self, r, dy, second):
        return self.slot(r, dy).at[pl.ds(self.half if second else 0, self.half)]

    def along_y(self, r):
        r = r % NZ
        self.send(8 + r, lambda r=r: self.slot(r), lambda: self.at.dev(0, 1))
        self.send(16 + r, lambda r=r: self.slot(r), lambda: self.at.dev(0, -1))

    def a(self, d):
        if d == 0:
            self.send(0, lambda: self.slot(0), lambda: self.at.dev(1))
            self.send(4, lambda: self.slot(0), lambda: self.at.dev(-1))
            self.along_y(0)
            return
        if d == 4:
            self.got(3, self.part(4, 0, False))
            self.got(7, self.part(4, 0, True))
            self.along_y(4)
            return
        self.got(d - 1, self.slot(-d))
        if d < 3:
            self.send(d, lambda: self.slot(-d), lambda: self.at.dev(1))
        else:
            self.send(3, lambda: self.part(-3, 0, False), lambda: self.at.dev(1))
        self.got(3 + d, self.slot(d))
        if d < 3:
            self.send(4 + d, lambda: self.slot(d), lambda: self.at.dev(-1))
        else:
            self.send(7, lambda: self.part(3, 0, True), lambda: self.at.dev(-1))
        self.along_y(-d)
        self.along_y(d)

    def each(self, d):
        return (0,) if d == 0 else (4,) if d == 4 else (d, NZ - d)

    def b(self, d):
        for r in self.each(d):
            self.got(8 + r, self.slot(r, -1))
            self.send(24 + r, lambda r=r: self.part(r, -1, False), lambda: self.at.dev(0, 1))
            self.got(16 + r, self.slot(r, 1))
            self.send(32 + r, lambda r=r: self.part(r, 1, True), lambda: self.at.dev(0, -1))

    def c(self, d):
        for r in self.each(d):
            self.got(24 + r, self.part(r, 2, False))
            self.got(32 + r, self.part(r, 2, True))
            self.send(40 + r, lambda r=r: self.buf.at[self.at.zat(r), :, self.at.core], lambda: self.at.dev(other=True))

    def w(self, d):
        for r in self.each(d):
            self.got(40 + r, self.buf.at[self.at.zat(r), :, 1 - self.at.core])


class YFirst(Mail):
    SEMS = 20

    def __init__(self, buf, half, *rest):
        super().__init__(*rest)
        self.buf, self.half = buf, half

    def slot(self, dy):
        return self.buf.at[self.at.z, self.at.yat(dy), self.at.core]

    def part(self, dy, second):
        return self.slot(dy).at[pl.ds(self.half if second else 0, self.half)]

    def column(self, r):
        return self.buf.at[self.at.zat(r), :, self.at.core]

    def pair(self, r, second):
        return self.buf.at[self.at.zat(r), pl.ds(2 if second else 0, 2), self.at.core]

    def over(self, r):
        self.send(12 + r % NZ, lambda r=r: self.column(r), lambda: self.at.dev(other=True))

    def s1(self):
        self.send(0, lambda: self.slot(0), lambda: self.at.dev(0, 1))
        self.send(1, lambda: self.slot(0), lambda: self.at.dev(0, -1))

    def s2(self):
        self.got(0, self.slot(-1))
        self.send(2, lambda: self.part(-1, False), lambda: self.at.dev(0, 1))
        self.got(1, self.slot(1))
        self.send(3, lambda: self.part(1, True), lambda: self.at.dev(0, -1))

    def s3(self):
        self.got(2, self.part(2, False))
        self.got(3, self.part(2, True))
        self.send(4, lambda: self.column(0), lambda: self.at.dev(1))
        self.send(8, lambda: self.column(0), lambda: self.at.dev(-1))
        self.over(0)

    def z(self, d):
        if d == 4:
            self.got(7, self.pair(4, False))
            self.got(11, self.pair(4, True))
            self.over(4)
            return
        self.got(3 + d, self.column(-d))
        if d < 3:
            self.send(4 + d, lambda: self.column(-d), lambda: self.at.dev(1))
        else:
            self.send(7, lambda: self.pair(-3, False), lambda: self.at.dev(1))
        self.got(7 + d, self.column(d))
        if d < 3:
            self.send(8 + d, lambda: self.column(d), lambda: self.at.dev(-1))
        else:
            self.send(11, lambda: self.pair(3, True), lambda: self.at.dev(-1))
        self.over(-d)
        self.over(d)

    def w(self):
        for r in range(NZ):
            self.got(12 + r, self.buf.at[self.at.zat(r), :, 1 - self.at.core])


def attend(kv, q_ref, s_scr, acc, peak, zs, h):
    tiles, width = 4, 256
    where = [(y, c) for y in range(NY) for c in range(NC)]

    def scores(j):
        top = None
        for a, (y, c) in enumerate(where):
            t = jnp.dot(
                kv[zs, y, c, 0:256, :],
                q_ref[h, :, j * width : (j + 1) * width],
                preferred_element_type=jnp.float32,
            )
            s_scr[j % 2, a * 256 : (a + 1) * 256, :] = t
            t = jnp.max(t.reshape(32, 8, width), axis=0)
            top = t if top is None else jnp.maximum(top, t)
        return top

    ones = jnp.ones((16, 256), jnp.bfloat16)
    later = scores(0)
    for j in range(tiles):
        top = later
        if j + 1 < tiles:
            later = scores(j + 1)
        cols = slice(j * width, (j + 1) * width)
        before = peak[h, 0:1, cols]
        now = jnp.maximum(before, jnp.max(top, axis=0, keepdims=True) * SCALE)
        peak[h, 0:1, cols] = now
        rescale = jnp.exp2(before - now)
        added = None
        for a, (y, c) in enumerate(where):
            exps = jnp.exp2(s_scr[j % 2, a * 256 : (a + 1) * 256, :] * SCALE - now)
            first = kv[zs, y, c, pl.ds(pl.multiple_of(256 + h * HD, HD), HD), :]
            second = kv[zs, y, c, pl.ds(pl.multiple_of(384 + h * HD, HD), HD), :]
            left = jnp.concatenate([jnp.concatenate([first, second], axis=1), ones], axis=0)
            term = jnp.dot(left, exps.astype(jnp.bfloat16), preferred_element_type=jnp.float32)
            added = term if added is None else added + term
        acc[h, :, cols] = acc[h, :, cols] * rescale + added


def gather_attend_kernel(
    q_ref, kv_in, up_in, down_in, o_ref, up_all, down_all,
    kv, s_scr, acc, peak, kv_s, kv_r, up_s, up_r, down_s, down_r, own_sem,
):
    at = Place()
    own = [
        pltpu.make_async_copy(src, dst.at[at.z, at.y, at.core], own_sem.at[k])
        for k, (src, dst) in enumerate(((kv_in, kv), (up_in, up_all), (down_in, down_all)))
    ]
    for copy in own:
        copy.start()
    barrier = pltpu.get_barrier_semaphore()
    for near in (at.dev(1), at.dev(-1), at.dev(0, 1), at.dev(0, -1), at.dev(other=True)):
        pl.semaphore_signal(barrier, inc=1, device_id={"sp": near}, device_id_type=MESH)
    acc[...] = jnp.zeros_like(acc)
    peak[...] = jnp.full_like(peak, -1e30)
    pl.semaphore_wait(barrier, 5)
    pair = ZFirst(kv, 256, at, kv_s, kv_r)
    up = YFirst(up_all, 16, at, up_s, up_r)
    down = ZFirst(down_all, 16, at, down_s, down_r)

    own[0].wait()
    pair.a(0)
    own[1].wait()
    own[2].wait()
    pair.b(0)
    pair.a(1)
    up.s1()
    pair.c(0)
    pair.w(0)
    polls = {
        1: (lambda: pair.b(1), lambda: pair.a(2), up.s2),
        2: (lambda: pair.c(1), up.s3, lambda: pair.w(1)),
        3: (lambda: pair.a(3),),
        4: (lambda: pair.b(2),),
        5: (lambda: pair.c(2), lambda: pair.a(4)),
        6: (lambda: up.z(1), lambda: down.a(0), lambda: pair.w(2)),
        7: (lambda: pair.b(3),),
        8: (lambda: pair.c(3), lambda: pair.b(4), lambda: down.a(1), lambda: down.b(0)),
        9: (lambda: pair.c(4),),
        10: (lambda: pair.w(3), lambda: up.z(2), lambda: down.a(2), lambda: down.b(1), lambda: down.c(0)),
        12: (lambda: down.a(3), lambda: down.b(2), lambda: down.c(1)),
        13: (lambda: pair.w(4),),
        14: (lambda: up.z(3), lambda: down.a(4), lambda: down.b(3), lambda: down.c(2)),
    }

    def step(n, carry):
        for k, todo in polls.items():

            @pl.when(n == k)
            def _(todo=todo):
                for do in todo:
                    do()

        turn = n // 2
        r = jnp.where(lax.rem(turn, 2) == 1, turn // 2 + 1, NZ - turn // 2)
        attend(kv, q_ref, s_scr, acc, peak, lax.rem(at.z + r, NZ), lax.rem(n, 2))
        return carry

    lax.fori_loop(0, 2 * NZ, step, 0)
    o_ref[...] = (acc[:, 0:HD, :] / acc[:, HD : HD + 1, :]).astype(jnp.bfloat16)
    down.b(4)
    down.c(3)
    up.z(4)
    down.c(4)
    up.w()
    for d in range(5):
        down.w(d)
    for mail in (pair, up, down):
        mail.finish()


def gather_attend(q_wide, kv_block, up_block, down_block):
    anywhere = pl.BlockSpec(memory_space=pl.ANY)
    vmem = pl.BlockSpec(memory_space=pltpu.VMEM)
    sems = [pltpu.SemaphoreType.DMA((n,)) for n in (48, 48, 20, 20, 48, 48, 3)]
    whole = jax.ShapeDtypeStruct((NZ, NY, NC, *up_block.shape), jnp.bfloat16)
    return pl.pallas_call(
        gather_attend_kernel,
        name="gather_attend",
        out_shape=(jax.ShapeDtypeStruct((2, HD, 1024), jnp.bfloat16), whole, whole),
        in_specs=[vmem, anywhere, anywhere, anywhere],
        out_specs=(vmem, anywhere, anywhere),
        scratch_shapes=[
            pltpu.VMEM((NZ, NY, NC, 512, 128), jnp.bfloat16),
            pltpu.VMEM((2, 2048, 256), jnp.float32),
            pltpu.VMEM((2, 80, 1024), jnp.float32),
            pltpu.VMEM((2, 8, 1024), jnp.float32),
            *sems,
        ],
        compiler_params=pltpu.CompilerParams(
            collective_id=0, has_side_effects=True, vmem_limit_bytes=56 * 1024 * 1024
        ),
    )(q_wide, kv_block, up_block, down_block)


def in_blocks(x, dim, count):
    dims = x.shape
    pieces = x.reshape(*dims[:dim], count, dims[dim] // count, *dims[dim + 1 :])
    return jnp.moveaxis(pieces, dim, 0)


def sum_at_owner(x, axis, dim):
    pieces = in_blocks(x, dim, lax.axis_size(axis))
    arrived = lax.all_to_all(pieces, axis, split_axis=0, concat_axis=0, tiled=True)
    return arrived.astype(jnp.float32).sum(axis=0)


def laid_out(pieces, dim):
    pieces = jnp.moveaxis(pieces, 0, dim)
    dims = pieces.shape
    return pieces.reshape(*dims[:dim], dims[dim] * dims[dim + 1], *dims[dim + 2 :])


def gather_directly(x, axis, dim):
    copies = jnp.broadcast_to(x, (lax.axis_size(axis), *x.shape))
    return laid_out(lax.all_to_all(copies, axis, split_axis=0, concat_axis=0, tiled=True), dim)


def shards(
    queries,
    keys,
    values,
    query_gain,
    key_gain,
    stream,
    out_weight,
    mixer_gain,
    up_weight,
    down_weight,
):
    rows = queries.shape[0]
    offset = lax.axis_index("sp") * rows
    pq = prepare(queries, query_gain, offset)
    pq = jnp.transpose(pq.reshape(rows, 2, 4, HD), (1, 3, 2, 0)).reshape(2, HD, 4 * rows)
    none = jnp.zeros((1, HD, 4 * rows), jnp.bfloat16)
    q_wide = jnp.concatenate(
        [jnp.concatenate([pq[:1], none], axis=1), jnp.concatenate([none, pq[1:]], axis=1)], axis=0
    )
    pk = prepare(keys, key_gain, offset).reshape(rows, 128)
    v_turned = jnp.transpose(values.reshape(2, 128, 128), (0, 2, 1)).reshape(256, 128)
    kv_block = jnp.concatenate([pk, v_turned], axis=0)
    out, up_all, down_all = gather_attend(q_wide, kv_block, up_weight, down_weight.T)
    head_out = jnp.transpose(out.reshape(2, HD, 4, rows), (3, 0, 2, 1)).reshape(rows, -1)

    partial_value = jnp.dot(head_out, out_weight, preferred_element_type=jnp.float32)
    model_width = partial_value.shape[1]
    share_cols = model_width // lax.axis_size("tp")
    first_col = lax.axis_index("tp") * share_cols
    share_sum = sum_at_owner(partial_value.astype(jnp.bfloat16), "tp", 1)
    own_stream = lax.dynamic_slice_in_dim(stream, first_col, share_cols, 1)
    own_mid = (own_stream.astype(jnp.float32) + share_sum).astype(jnp.bfloat16)
    own_wide = own_mid.astype(jnp.float32)
    squares = lax.psum(jnp.sum(own_wide * own_wide, axis=-1), "tp")
    own_gain = lax.dynamic_slice_in_dim(mixer_gain, first_col, share_cols, 0)
    normed_part = own_wide * lax.rsqrt(squares / model_width + EPSILON)[:, None] * own_gain
    normed = gather_directly(normed_part.astype(jnp.bfloat16), "tp", 1)
    up_whole = up_all.reshape(model_width, -1)
    up_sums = jnp.dot(normed, up_whole, preferred_element_type=jnp.float32)
    hidden = jnp.square(jax.nn.relu(up_sums)).astype(jnp.bfloat16)
    down_turned = down_all.reshape(model_width, -1)
    down_part = lax.dot_general(
        hidden, down_turned, (((1,), (1,)), ((), ())), preferred_element_type=jnp.float32
    )
    down_share = sum_at_owner(down_part.astype(jnp.bfloat16), "tp", 1)
    return (own_mid.astype(jnp.float32) + down_share).astype(jnp.bfloat16)


def solution(mesh):
    return jax.shard_map(
        shards,
        mesh=mesh,
        in_specs=(
            P("sp", "tp"),
            P("sp", "tp"),
            P("sp", "tp"),
            P(),
            P(),
            P("sp", None),
            P("tp", None),
            P(),
            P("sp", "tp"),
            P("tp", "sp"),
        ),
        out_specs=P("sp", "tp"),
        check_vma=False,
    )
```

```python
import math

import jax
import jax.numpy as jnp
from jax import lax
from jax.experimental import pallas as pl
from jax.experimental.pallas import tpu as pltpu
from jax.sharding import PartitionSpec as P

HD = 64
GRID_W = 64
EPSILON = 1e-06
NX, NZ, NY, NC = 4, 8, 4, 2
SCALE = math.log2(math.e) / math.sqrt(HD)
MESH = pl.DeviceIdType.MESH


def prepare(projected, gain_vec, offset):
    row_count = projected.shape[0]
    head_count = projected.shape[1] // HD
    widened = projected.astype(jnp.float32).reshape(row_count, head_count, HD)
    widened = (
        widened
        * lax.rsqrt(jnp.mean(widened * widened, axis=-1, keepdims=True) + EPSILON)
        * gain_vec
    )
    position = offset + jnp.arange(row_count, dtype=jnp.int32)
    grid_row = (position // GRID_W).astype(jnp.float32)
    grid_col = (position % GRID_W).astype(jnp.float32)
    half_dim = HD // 2
    inverse = 1.0 / jnp.power(10000.0, jnp.arange(0, half_dim, 2, dtype=jnp.float32) / half_dim)
    angle = jnp.concatenate([grid_row[:, None] * inverse, grid_col[:, None] * inverse], axis=-1)
    cosine = jnp.cos(angle)[:, None, :]
    sine_table = jnp.sin(angle)[:, None, :]
    paired = widened.reshape(row_count, head_count, half_dim, 2)
    former = paired[..., 0]
    latter = paired[..., 1]
    rotated = jnp.stack(
        [former * cosine - latter * sine_table, former * sine_table + latter * cosine], axis=-1
    )
    return rotated.reshape(row_count, head_count, HD).astype(jnp.bfloat16)


class Place:
    def __init__(self):
        me = lax.axis_index("sp")
        self.core = lax.rem(me, NC)
        self.y = lax.rem(me // NC, NY)
        self.z = me // (NC * NY)
        self.x = lax.axis_index("tp")

    def yat(self, d):
        return lax.rem(self.y + (d + NY) % NY, NY)

    def xat(self, d):
        return lax.rem(self.x + (d + NX) % NX, NX)

    def dev(self, dz=0, dy=0):
        return {"sp": (lax.rem(self.z + (dz + NZ) % NZ, NZ) * NY + self.yat(dy)) * NC + self.core}

    def other(self):
        return {"sp": (self.z * NY + self.y) * NC + 1 - self.core}

    def along(self, dx):
        return {"tp": self.xat(dx)}


class Mail:
    def __init__(self, place, send_sems, recv_sems):
        self.at, self.ss, self.rs, self.sent = place, send_sems, recv_sems, []

    def copy(self, key, src, dst, target):
        return pltpu.make_async_remote_copy(
            src_ref=src,
            dst_ref=dst,
            send_sem=self.ss.at[key],
            recv_sem=self.rs.at[key],
            device_id=target,
            device_id_type=MESH,
        )

    def send(self, key, src, dst, target):
        self.copy(key, src(), dst(), target()).start()
        self.sent.append((key, src, dst, target))

    def got(self, key, ref):
        self.copy(key, ref, ref, self.at.other()).wait_recv()

    def finish(self):
        for key, src, dst, target in self.sent:
            self.copy(key, src(), dst(), target()).wait_send()


class Around(Mail):
    SEMS = 7

    def __init__(self, own, buf, half, *rest):
        super().__init__(*rest)
        self.own, self.buf, self.half = own, buf, half

    def slot(self, k):
        return self.buf.at[k, self.at.core]

    def part(self, k, second):
        return self.buf.at[k, self.at.core, pl.ds(self.half if second else 0, self.half)]

    def over(self, k):
        self.send(3 + k, lambda: self.slot(k), lambda: self.slot(k), self.at.other)

    def s1(self):
        own = lambda: self.own.at[self.at.core]
        self.send(0, own, lambda: self.slot(1), lambda: self.at.along(1))
        self.send(1, own, lambda: self.slot(2), lambda: self.at.along(-1))

    def s2(self):
        self.got(0, self.slot(1))
        self.send(2, lambda: self.part(1, False), lambda: self.part(3, False), lambda: self.at.along(1))
        self.got(1, self.slot(2))
        self.send(3, lambda: self.part(2, True), lambda: self.part(3, True), lambda: self.at.along(-1))
        self.over(1)
        self.over(2)

    def s3(self):
        self.got(2, self.part(3, False))
        self.got(3, self.part(3, True))
        self.over(3)

    def w(self):
        for k in (1, 2, 3):
            self.got(3 + k, self.buf.at[k, 1 - self.at.core])


class ZFirst(Mail):
    SEMS = 33

    def __init__(self, own, buf, half, *rest):
        super().__init__(*rest)
        self.own, self.buf, self.half = own, buf, half

    def slot(self, k):
        return self.buf.at[k, self.at.y, self.at.core]

    def part(self, k, dy, second):
        return self.buf.at[k, self.at.yat(dy), self.at.core, pl.ds(self.half if second else 0, self.half)]

    def slots(self, d):
        return pl.ds(0, 1) if d == 0 else pl.ds(7, 1) if d == 4 else pl.ds(2 * d - 1, 2)

    def pair(self, d, dy=0):
        return self.buf.at[self.slots(d), self.at.yat(dy), self.at.core]

    def columns(self, d, other=False):
        core = 1 - self.at.core if other else self.at.core
        return self.buf.at[self.slots(d), :, core]

    def along_y(self, d):
        self.send(8 + d, lambda: self.pair(d), lambda: self.pair(d), lambda: self.at.dev(0, 1))
        self.send(13 + d, lambda: self.pair(d), lambda: self.pair(d), lambda: self.at.dev(0, -1))

    def a(self, d):
        if d == 0:
            self.send(8, lambda: self.own, lambda: self.slot(0), lambda: self.at.dev(0, 1))
            self.send(13, lambda: self.own, lambda: self.slot(0), lambda: self.at.dev(0, -1))
            self.send(0, lambda: self.own, lambda: self.slot(2), lambda: self.at.dev(1))
            self.send(4, lambda: self.own, lambda: self.slot(1), lambda: self.at.dev(-1))
            return
        if d == 4:
            self.got(3, self.part(7, 0, False))
            self.got(7, self.part(7, 0, True))
        else:
            low, high = 2 * d, 2 * d - 1
            self.got(d - 1, self.slot(low))
            if d < 3:
                self.send(d, lambda: self.slot(low), lambda: self.slot(low + 2), lambda: self.at.dev(1))
            else:
                self.send(3, lambda: self.part(6, 0, False), lambda: self.part(7, 0, False), lambda: self.at.dev(1))
            self.got(3 + d, self.slot(high))
            if d < 3:
                self.send(4 + d, lambda: self.slot(high), lambda: self.slot(high + 2), lambda: self.at.dev(-1))
            else:
                self.send(7, lambda: self.part(5, 0, True), lambda: self.part(7, 0, True), lambda: self.at.dev(-1))
        self.along_y(d)

    def piece(self, d, dy, second):
        if d in (0, 4):
            return self.part(0 if d == 0 else 7, dy, second)
        return self.buf.at[2 * d if second else 2 * d - 1, self.at.yat(dy), self.at.core]

    def b(self, d):
        self.got(8 + d, self.pair(d, -1))
        one = lambda: self.piece(d, -1, False)
        self.send(18 + d, one, one, lambda: self.at.dev(0, 1))
        self.got(13 + d, self.pair(d, 1))
        two = lambda: self.piece(d, 1, True)
        self.send(23 + d, two, two, lambda: self.at.dev(0, -1))

    def c(self, d):
        self.got(18 + d, self.piece(d, 2, False))
        self.got(23 + d, self.piece(d, 2, True))
        self.send(28 + d, lambda: self.columns(d), lambda: self.columns(d), self.at.other)

    def w(self, d):
        self.got(28 + d, self.columns(d, True))


class YFirst(Mail):
    SEMS = 17

    def __init__(self, own, buf, half, *rest):
        super().__init__(*rest)
        self.own, self.buf, self.half = own, buf, half

    def slot(self, dy):
        return self.buf.at[0, self.at.yat(dy), self.at.core]

    def part(self, dy, second):
        return self.slot(dy).at[pl.ds(self.half if second else 0, self.half)]

    def column(self, k):
        return self.buf.at[k, :, self.at.core]

    def two(self, k, second):
        return self.buf.at[k, pl.ds(2 if second else 0, 2), self.at.core]

    def columns(self, d, other=False):
        core = 1 - self.at.core if other else self.at.core
        return self.buf.at[pl.ds(0, 1) if d == 0 else pl.ds(7, 1) if d == 4 else pl.ds(2 * d - 1, 2), :, core]

    def over(self, d):
        self.send(12 + d, lambda: self.columns(d), lambda: self.columns(d), self.at.other)

    def s1(self):
        self.send(0, lambda: self.own, lambda: self.slot(0), lambda: self.at.dev(0, 1))
        self.send(1, lambda: self.own, lambda: self.slot(0), lambda: self.at.dev(0, -1))

    def s2(self):
        self.got(0, self.slot(-1))
        one = lambda: self.part(-1, False)
        self.send(2, one, one, lambda: self.at.dev(0, 1))
        self.got(1, self.slot(1))
        two = lambda: self.part(1, True)
        self.send(3, two, two, lambda: self.at.dev(0, -1))

    def s3(self):
        self.got(2, self.part(2, False))
        self.got(3, self.part(2, True))
        self.send(4, lambda: self.column(0), lambda: self.column(2), lambda: self.at.dev(1))
        self.send(8, lambda: self.column(0), lambda: self.column(1), lambda: self.at.dev(-1))
        self.over(0)

    def z(self, d):
        if d == 4:
            self.got(7, self.two(7, False))
            self.got(11, self.two(7, True))
            self.over(4)
            return
        low, high = 2 * d, 2 * d - 1
        self.got(3 + d, self.column(low))
        if d < 3:
            self.send(4 + d, lambda: self.column(low), lambda: self.column(low + 2), lambda: self.at.dev(1))
        else:
            self.send(7, lambda: self.two(6, False), lambda: self.two(7, False), lambda: self.at.dev(1))
        self.got(7 + d, self.column(high))
        if d < 3:
            self.send(8 + d, lambda: self.column(high), lambda: self.column(high + 2), lambda: self.at.dev(-1))
        else:
            self.send(11, lambda: self.two(5, True), lambda: self.two(7, True), lambda: self.at.dev(-1))
        self.over(d)

    def w(self):
        for d in range(5):
            self.got(12 + d, self.columns(d, True))


def attend(kv, q_ref, s_scr, acc, peak, zs, h):
    tiles, width = 4, 256
    where = [(y, c) for y in range(NY) for c in range(NC)]

    def scores(j):
        top = None
        for a, (y, c) in enumerate(where):
            t = jnp.dot(
                kv[zs, y, c, 0:256, :],
                q_ref[h, :, j * width : (j + 1) * width],
                preferred_element_type=jnp.float32,
            )
            s_scr[j % 2, a * 256 : (a + 1) * 256, :] = t
            t = jnp.max(t.reshape(32, 8, width), axis=0)
            top = t if top is None else jnp.maximum(top, t)
        return top

    ones = jnp.ones((16, 256), jnp.bfloat16)
    later = scores(0)
    for j in range(tiles):
        top = later
        if j + 1 < tiles:
            later = scores(j + 1)
        cols = slice(j * width, (j + 1) * width)
        before = peak[h, 0:1, cols]
        now = jnp.maximum(before, jnp.max(top, axis=0, keepdims=True) * SCALE)
        peak[h, 0:1, cols] = now
        rescale = jnp.exp2(before - now)
        added = None
        for a, (y, c) in enumerate(where):
            exps = jnp.exp2(s_scr[j % 2, a * 256 : (a + 1) * 256, :] * SCALE - now)
            first = kv[zs, y, c, pl.ds(pl.multiple_of(256 + h * HD, HD), HD), :]
            second = kv[zs, y, c, pl.ds(pl.multiple_of(384 + h * HD, HD), HD), :]
            left = jnp.concatenate([jnp.concatenate([first, second], axis=1), ones], axis=0)
            term = jnp.dot(left, exps.astype(jnp.bfloat16), preferred_element_type=jnp.float32)
            added = term if added is None else added + term
        acc[h, :, cols] = acc[h, :, cols] * rescale + added


def layer_kernel(
    q_ref, kv_in, up_in, down_in, ow_in, stream, gain, o_ref,
    kv, up, down, ow, s_scr, acc, peak, st, heads, mid, nrm, hid, part, arrived, transit,
    kv_s, kv_r, up_s, up_r, down_s, down_r, ow_s, ow_r, tp_s, tp_r, own_sem,
):
    at = Place()
    own = [
        pltpu.make_async_copy(src, dst, own_sem.at[k])
        for k, (src, dst) in enumerate(
            (
                (kv_in, kv.at[0, at.y, at.core]),
                (up_in, up.at[0, at.y, at.core]),
                (down_in, down.at[0, at.y, at.core]),
                (ow_in, ow.at[0]),
                (stream.at[at.x], st),
            )
        )
    ]
    for copy in own:
        copy.start()
    barrier = pltpu.get_barrier_semaphore()
    nearby = [at.dev(1), at.dev(-1), at.dev(0, 1), at.dev(0, -1), at.other()]
    nearby += [at.along(1), at.along(-1), at.along(2)]
    for near in nearby:
        pl.semaphore_signal(barrier, inc=1, device_id=near, device_id_type=MESH)
    acc[...] = jnp.zeros_like(acc)
    peak[...] = jnp.full_like(peak, -1e30)
    pl.semaphore_wait(barrier, len(nearby))
    pairs = ZFirst(kv_in, kv, 256, at, kv_s, kv_r)
    ups = YFirst(up_in, up, 16, at, up_s, up_r)
    downs = ZFirst(down_in, down, 16, at, down_s, down_r)
    outs = Around(ow_in, ow, 128, at, ow_s, ow_r)
    across = Mail(at, tp_s, tp_r)

    pairs.a(0)
    ups.s1()
    outs.s1()
    own[0].wait()
    pairs.b(0)
    pairs.a(1)
    pairs.c(0)
    pairs.w(0)
    polls = {
        1: (lambda: pairs.b(1), lambda: pairs.a(2), ups.s2),
        2: (lambda: pairs.c(1), own[1].wait, ups.s3, lambda: pairs.w(1)),
        4: (lambda: pairs.b(2), lambda: pairs.a(3)),
        5: (lambda: pairs.c(2), lambda: pairs.a(4), lambda: downs.a(0)),
        6: (lambda: pairs.w(2), lambda: ups.z(1), lambda: downs.a(1)),
        7: (lambda: pairs.b(3),),
        8: (lambda: pairs.c(3), lambda: pairs.b(4), lambda: downs.a(2)),
        9: (lambda: pairs.c(4), lambda: downs.b(0), outs.s2),
        10: (lambda: pairs.w(3), lambda: ups.z(2), lambda: downs.b(1), own[2].wait, lambda: downs.c(0)),
        11: (lambda: downs.a(3),),
        12: (lambda: downs.b(2), lambda: downs.c(1)),
        13: (lambda: downs.a(4), outs.s3),
        14: (lambda: pairs.w(4), lambda: ups.z(3)),
        15: (lambda: downs.b(3), lambda: downs.c(2)),
    }

    def step(n, carry):
        for k, todo in polls.items():

            @pl.when(n == k)
            def _(todo=todo):
                for do in todo:
                    do()

        attend(kv, q_ref, s_scr, acc, peak, n // 2, lax.rem(n, 2))
        return carry

    lax.fori_loop(0, 2 * NZ, step, 0)

    for k in range(4):
        sides = []
        for g in (2 * k, 2 * k + 1):
            h, cols = g // 4, slice(g % 4 * 256, (g % 4 + 1) * 256)
            sides.append(jnp.transpose(acc[h, 0:HD, cols] / acc[h, HD : HD + 1, cols]))
        both = jnp.concatenate(sides, axis=1).astype(jnp.bfloat16)
        heads[0, :, :, k * 128 : (k + 1) * 128] = both.reshape(NX, 64, 128)
    offsets = (0, -1, 1, 2)
    own[3].wait()
    own[4].wait()
    outs.w()
    across.send(2, lambda: heads.at[0, at.xat(2)], lambda: heads.at[1, 2], lambda: at.along(2))
    across.send(0, lambda: heads.at[0, at.xat(1)], lambda: heads.at[1, 0], lambda: at.along(1))
    across.send(1, lambda: heads.at[0, at.xat(-1)], lambda: heads.at[1, 1], lambda: at.along(-1))
    downs.b(4)
    downs.c(3)
    for k in range(3):
        across.got(k, heads.at[1, k])
    lefts = [heads[0, at.x], heads[1, 0], heads[1, 1], heads[1, 2]]
    for j in range(5):
        if j < 4:
            cols = slice(j * 512, (j + 1) * 512)
            attended = None
            for i, left in enumerate(lefts):
                term = jnp.dot(left[:, 0:256], ow[i, 0, :, cols], preferred_element_type=jnp.float32)
                term += jnp.dot(left[:, 256:512], ow[i, 1, :, cols], preferred_element_type=jnp.float32)
                term = term.astype(jnp.bfloat16).astype(jnp.float32)
                attended = term if attended is None else attended + term
            mid[at.x, j] = (st[:, cols].astype(jnp.float32) + attended).astype(jnp.bfloat16)
        if j > 0:
            chunk = lambda j=j: mid.at[at.x, j - 1]
            across.send(3 + j - 1, chunk, chunk, lambda: at.along(1))
            across.send(7 + j - 1, chunk, chunk, lambda: at.along(-1))

    def norm(i):
        rows = jnp.concatenate([mid[at.xat(offsets[i]), j] for j in range(4)], axis=1)
        rows = rows.astype(jnp.float32)
        mean = jnp.mean(rows * rows, axis=-1, keepdims=True)
        nrm[i * 64 : (i + 1) * 64, :] = (rows * lax.rsqrt(mean + EPSILON) * gain[...]).astype(jnp.bfloat16)

    def slot_z(k):
        return at.z if k == 0 else lax.rem(at.z + (4 if k == 7 else (k + 1) // 2 if k % 2 else NZ - k // 2), NZ)

    def lift(first, last):
        rows = slice(first * 64, last * 64)
        for t in range(4):
            cols = slice(t * 512, (t + 1) * 512)
            sums = None
            for k in range(NZ):
                left = nrm[rows, pl.ds(pl.multiple_of(slot_z(k) * 256, 256), 256)]
                term = jnp.dot(left, up[k, :, :, :, cols].reshape(256, 512), preferred_element_type=jnp.float32)
                sums = term if sums is None else sums + term
            hid[rows, cols] = jnp.square(jnp.maximum(sums, 0.0)).astype(jnp.bfloat16)

    norm(0)
    for j in (0, 1):
        chunk = lambda j=j: mid.at[at.xat(-1), j]
        across.got(3 + j, chunk())
        across.send(11 + j, chunk, chunk, lambda: at.along(1))
    for j in (2, 3):
        chunk = lambda j=j: mid.at[at.xat(1), j]
        across.got(7 + j, chunk())
        across.send(11 + j, chunk, chunk, lambda: at.along(-1))
    ups.z(4)
    downs.c(4)
    ups.w()
    lift(0, 1)
    for j in (2, 3):
        across.got(3 + j, mid.at[at.xat(-1), j])
    for j in (0, 1):
        across.got(7 + j, mid.at[at.xat(1), j])
    norm(1)
    norm(2)
    lift(1, 3)
    for j in range(4):
        across.got(11 + j, mid.at[at.xat(2), j])
    norm(3)
    lift(3, 4)
    for d in range(5):
        downs.w(d)

    def lower(k):
        for t in range(2):
            r = lax.rem(2 * at.xat(k) + t + NZ - at.z, NZ)
            where = jnp.where(r > 4, 2 * (NZ - r), jnp.maximum(2 * r - 1, 0))
            sums = lax.dot_general(
                hid[...],
                down[where].reshape(256, 2048),
                (((1,), (1,)), ((), ())),
                preferred_element_type=jnp.float32,
            ).astype(jnp.bfloat16)
            for i in range(4):
                part[k, at.xat(offsets[i]), :, t * 256 : (t + 1) * 256] = sums[i * 64 : (i + 1) * 64]

    lower(2)
    lower(1)
    across.send(15, lambda: part.at[2, pl.ds(0, 2)], lambda: transit.at[0], lambda: at.along(1))
    across.send(16, lambda: part.at[2, pl.ds(2, 2)], lambda: transit.at[1], lambda: at.along(-1))
    lower(3)
    across.send(17, lambda: part.at[1], lambda: arrived.at[0], lambda: at.along(1))
    lower(0)
    across.send(18, lambda: part.at[3], lambda: arrived.at[1], lambda: at.along(-1))
    across.got(15, transit.at[0])
    across.send(19, lambda: transit.at[0], lambda: arrived.at[2, pl.ds(0, 2)], lambda: at.along(1))
    across.got(16, transit.at[1])
    across.send(20, lambda: transit.at[1], lambda: arrived.at[2, pl.ds(2, 2)], lambda: at.along(-1))
    across.got(17, arrived.at[0])
    across.got(18, arrived.at[1])
    across.got(19, arrived.at[2, pl.ds(0, 2)])
    across.got(20, arrived.at[2, pl.ds(2, 2)])
    for s in range(4):
        total = part[0, s].astype(jnp.float32)
        for k in range(3):
            total += arrived[k, s].astype(jnp.float32)
        o_ref[s] = (mid[s, at.x].astype(jnp.float32) + total).astype(jnp.bfloat16)
    for mail in (pairs, ups, downs, outs, across):
        mail.finish()


def layer(*operands):
    anywhere = pl.BlockSpec(memory_space=pl.ANY)
    vmem = pl.BlockSpec(memory_space=pltpu.VMEM)
    bf16, f32 = jnp.bfloat16, jnp.float32
    held = [
        ((NZ, NY, NC, 512, 128), bf16),
        ((NZ, NY, NC, 32, 2048), bf16),
        ((NZ, NY, NC, 32, 2048), bf16),
        ((NX, 2, 256, 2048), bf16),
        ((2, 2048, 256), f32),
        ((2, 80, 1024), f32),
        ((2, 8, 1024), f32),
        ((64, 2048), bf16),
        ((2, NX, 64, 512), bf16),
        ((NX, 4, 64, 512), bf16),
        ((256, 2048), bf16),
        ((256, 2048), bf16),
        ((NX, NX, 64, 512), bf16),
        ((3, NX, 64, 512), bf16),
        ((2, 2, 64, 512), bf16),
    ]
    counts = (33, 33, 17, 17, 33, 33, 7, 7, 21, 21, 5)
    return pl.pallas_call(
        layer_kernel,
        name="layer",
        out_shape=jax.ShapeDtypeStruct((NX, 64, 512), bf16),
        in_specs=[vmem, anywhere, anywhere, anywhere, anywhere, anywhere, vmem],
        out_specs=vmem,
        scratch_shapes=[
            *(pltpu.VMEM(shape, kind) for shape, kind in held),
            *(pltpu.SemaphoreType.DMA((n,)) for n in counts),
        ],
        compiler_params=pltpu.CompilerParams(
            collective_id=0, has_side_effects=True, vmem_limit_bytes=60 * 1024 * 1024
        ),
    )(*operands)


def shards(
    queries,
    keys,
    values,
    query_gain,
    key_gain,
    stream,
    out_weight,
    mixer_gain,
    up_weight,
    down_weight,
):
    rows = queries.shape[0]
    offset = lax.axis_index("sp") * rows
    pq = prepare(queries, query_gain, offset)
    pq = jnp.transpose(pq.reshape(rows, 2, 4, HD), (1, 3, 2, 0)).reshape(2, HD, 4 * rows)
    none = jnp.zeros((1, HD, 4 * rows), jnp.bfloat16)
    q_wide = jnp.concatenate(
        [jnp.concatenate([pq[:1], none], axis=1), jnp.concatenate([none, pq[1:]], axis=1)], axis=0
    )
    pk = prepare(keys, key_gain, offset).reshape(rows, 128)
    v_turned = jnp.transpose(values.reshape(2, 128, 128), (0, 2, 1)).reshape(256, 128)
    kv_block = jnp.concatenate([pk, v_turned], axis=0)
    out_block = out_weight.reshape(2, 256, -1)
    width = stream.shape[1]
    updated = layer(
        q_wide,
        kv_block,
        up_weight,
        down_weight.T,
        out_block,
        stream.reshape(NX, rows // NX, width),
        mixer_gain.reshape(1, width),
    )
    return updated.reshape(rows, -1)


def solution(mesh):
    return jax.shard_map(
        shards,
        mesh=mesh,
        in_specs=(
            P("sp", "tp"),
            P("sp", "tp"),
            P("sp", "tp"),
            P(),
            P(),
            P("sp", None),
            P("tp", None),
            P(),
            P("sp", "tp"),
            P("tp", "sp"),
        ),
        out_specs=P("sp", "tp"),
        check_vma=False,
    )
```

```python
import math

import jax
import jax.numpy as jnp
from jax import lax
from jax.experimental import pallas as pl
from jax.experimental.pallas import tpu as pltpu
from jax.sharding import PartitionSpec as P

HD = 64
GRID_W = 64
EPSILON = 1e-06
NX, NZ, NY, NC = 4, 8, 4, 2
SCALE = math.log2(math.e) / math.sqrt(HD)
MESH = pl.DeviceIdType.MESH


def prepare(projected, gain_vec, offset):
    row_count = projected.shape[0]
    head_count = projected.shape[1] // HD
    widened = projected.astype(jnp.float32).reshape(row_count, head_count, HD)
    widened = (
        widened
        * lax.rsqrt(jnp.mean(widened * widened, axis=-1, keepdims=True) + EPSILON)
        * gain_vec
    )
    position = offset + jnp.arange(row_count, dtype=jnp.int32)
    grid_row = (position // GRID_W).astype(jnp.float32)
    grid_col = (position % GRID_W).astype(jnp.float32)
    half_dim = HD // 2
    inverse = 1.0 / jnp.power(10000.0, jnp.arange(0, half_dim, 2, dtype=jnp.float32) / half_dim)
    angle = jnp.concatenate([grid_row[:, None] * inverse, grid_col[:, None] * inverse], axis=-1)
    cosine = jnp.cos(angle)[:, None, :]
    sine_table = jnp.sin(angle)[:, None, :]
    paired = widened.reshape(row_count, head_count, half_dim, 2)
    former = paired[..., 0]
    latter = paired[..., 1]
    rotated = jnp.stack(
        [former * cosine - latter * sine_table, former * sine_table + latter * cosine], axis=-1
    )
    return rotated.reshape(row_count, head_count, HD).astype(jnp.bfloat16)


class Place:
    def __init__(self):
        me = lax.axis_index("sp")
        self.core = lax.rem(me, NC)
        self.y = lax.rem(me // NC, NY)
        self.z = me // (NC * NY)
        self.x = lax.axis_index("tp")

    def yat(self, d):
        return lax.rem(self.y + (d + NY) % NY, NY)

    def xat(self, d):
        return lax.rem(self.x + (d + NX) % NX, NX)

    def dev(self, dz=0, dy=0):
        return {"sp": (lax.rem(self.z + (dz + NZ) % NZ, NZ) * NY + self.yat(dy)) * NC + self.core}

    def other(self):
        return {"sp": (self.z * NY + self.y) * NC + 1 - self.core}

    def along(self, dx):
        return {"tp": self.xat(dx)}


class Mail:
    def __init__(self, place, send_sems, recv_sems):
        self.at, self.ss, self.rs, self.sent = place, send_sems, recv_sems, []

    def copy(self, key, src, dst, target):
        return pltpu.make_async_remote_copy(
            src_ref=src,
            dst_ref=dst,
            send_sem=self.ss.at[key],
            recv_sem=self.rs.at[key],
            device_id=target,
            device_id_type=MESH,
        )

    def send(self, key, src, dst, target):
        self.copy(key, src(), dst(), target()).start()
        self.sent.append((key, src, dst, target))

    def got(self, key, ref):
        self.copy(key, ref, ref, self.at.other()).wait_recv()

    def finish(self):
        for key, src, dst, target in self.sent:
            self.copy(key, src(), dst(), target()).wait_send()


class Around(Mail):
    SEMS = 7

    def __init__(self, own, buf, half, *rest):
        super().__init__(*rest)
        self.own, self.buf, self.half = own, buf, half

    def slot(self, k):
        return self.buf.at[k, self.at.core]

    def part(self, k, second):
        return self.buf.at[k, self.at.core, pl.ds(self.half if second else 0, self.half)]

    def over(self, k):
        self.send(3 + k, lambda: self.slot(k), lambda: self.slot(k), self.at.other)

    def s1(self):
        own = lambda: self.own.at[self.at.core]
        self.send(0, own, lambda: self.slot(1), lambda: self.at.along(1))
        self.send(1, own, lambda: self.slot(2), lambda: self.at.along(-1))

    def s2(self):
        self.got(0, self.slot(1))
        self.send(2, lambda: self.part(1, False), lambda: self.part(3, False), lambda: self.at.along(1))
        self.got(1, self.slot(2))
        self.send(3, lambda: self.part(2, True), lambda: self.part(3, True), lambda: self.at.along(-1))
        self.over(1)
        self.over(2)

    def s3(self):
        self.got(2, self.part(3, False))
        self.got(3, self.part(3, True))
        self.over(3)

    def w(self):
        for k in (1, 2, 3):
            self.got(3 + k, self.buf.at[k, 1 - self.at.core])


class ZFirst(Mail):
    SEMS = 33

    def __init__(self, own, buf, half, *rest):
        super().__init__(*rest)
        self.own, self.buf, self.half = own, buf, half

    def slot(self, k):
        return self.buf.at[k, self.at.y, self.at.core]

    def part(self, k, dy, second):
        return self.buf.at[k, self.at.yat(dy), self.at.core, pl.ds(self.half if second else 0, self.half)]

    def slots(self, d):
        return pl.ds(0, 1) if d == 0 else pl.ds(7, 1) if d == 4 else pl.ds(2 * d - 1, 2)

    def pair(self, d, dy=0):
        return self.buf.at[self.slots(d), self.at.yat(dy), self.at.core]

    def columns(self, d, other=False):
        core = 1 - self.at.core if other else self.at.core
        return self.buf.at[self.slots(d), :, core]

    def along_y(self, d):
        self.send(8 + d, lambda: self.pair(d), lambda: self.pair(d), lambda: self.at.dev(0, 1))
        self.send(13 + d, lambda: self.pair(d), lambda: self.pair(d), lambda: self.at.dev(0, -1))

    def a(self, d):
        if d == 0:
            self.send(8, lambda: self.own, lambda: self.slot(0), lambda: self.at.dev(0, 1))
            self.send(13, lambda: self.own, lambda: self.slot(0), lambda: self.at.dev(0, -1))
            self.send(0, lambda: self.own, lambda: self.slot(2), lambda: self.at.dev(1))
            self.send(4, lambda: self.own, lambda: self.slot(1), lambda: self.at.dev(-1))
            return
        if d == 4:
            self.got(3, self.part(7, 0, False))
            self.got(7, self.part(7, 0, True))
        else:
            low, high = 2 * d, 2 * d - 1
            self.got(d - 1, self.slot(low))
            if d < 3:
                self.send(d, lambda: self.slot(low), lambda: self.slot(low + 2), lambda: self.at.dev(1))
            else:
                self.send(3, lambda: self.part(6, 0, False), lambda: self.part(7, 0, False), lambda: self.at.dev(1))
            self.got(3 + d, self.slot(high))
            if d < 3:
                self.send(4 + d, lambda: self.slot(high), lambda: self.slot(high + 2), lambda: self.at.dev(-1))
            else:
                self.send(7, lambda: self.part(5, 0, True), lambda: self.part(7, 0, True), lambda: self.at.dev(-1))
        self.along_y(d)

    def piece(self, d, dy, second):
        if d in (0, 4):
            return self.part(0 if d == 0 else 7, dy, second)
        return self.buf.at[2 * d if second else 2 * d - 1, self.at.yat(dy), self.at.core]

    def b(self, d):
        self.got(8 + d, self.pair(d, -1))
        one = lambda: self.piece(d, -1, False)
        self.send(18 + d, one, one, lambda: self.at.dev(0, 1))
        self.got(13 + d, self.pair(d, 1))
        two = lambda: self.piece(d, 1, True)
        self.send(23 + d, two, two, lambda: self.at.dev(0, -1))

    def c(self, d):
        self.got(18 + d, self.piece(d, 2, False))
        self.got(23 + d, self.piece(d, 2, True))
        self.send(28 + d, lambda: self.columns(d), lambda: self.columns(d), self.at.other)

    def w(self, d):
        self.got(28 + d, self.columns(d, True))


class YFirst(Mail):
    SEMS = 17

    def __init__(self, own, buf, half, *rest):
        super().__init__(*rest)
        self.own, self.buf, self.half = own, buf, half

    def slot(self, dy):
        return self.buf.at[0, self.at.yat(dy), self.at.core]

    def part(self, dy, second):
        return self.slot(dy).at[pl.ds(self.half if second else 0, self.half)]

    def column(self, k):
        return self.buf.at[k, :, self.at.core]

    def two(self, k, second):
        return self.buf.at[k, pl.ds(2 if second else 0, 2), self.at.core]

    def columns(self, d, other=False):
        core = 1 - self.at.core if other else self.at.core
        return self.buf.at[pl.ds(0, 1) if d == 0 else pl.ds(7, 1) if d == 4 else pl.ds(2 * d - 1, 2), :, core]

    def over(self, d):
        self.send(12 + d, lambda: self.columns(d), lambda: self.columns(d), self.at.other)

    def s1(self):
        self.send(0, lambda: self.own, lambda: self.slot(0), lambda: self.at.dev(0, 1))
        self.send(1, lambda: self.own, lambda: self.slot(0), lambda: self.at.dev(0, -1))

    def s2(self):
        self.got(0, self.slot(-1))
        one = lambda: self.part(-1, False)
        self.send(2, one, one, lambda: self.at.dev(0, 1))
        self.got(1, self.slot(1))
        two = lambda: self.part(1, True)
        self.send(3, two, two, lambda: self.at.dev(0, -1))

    def s3(self):
        self.got(2, self.part(2, False))
        self.got(3, self.part(2, True))
        self.send(4, lambda: self.column(0), lambda: self.column(2), lambda: self.at.dev(1))
        self.send(8, lambda: self.column(0), lambda: self.column(1), lambda: self.at.dev(-1))
        self.over(0)

    def z(self, d):
        if d == 4:
            self.got(7, self.two(7, False))
            self.got(11, self.two(7, True))
            self.over(4)
            return
        low, high = 2 * d, 2 * d - 1
        self.got(3 + d, self.column(low))
        if d < 3:
            self.send(4 + d, lambda: self.column(low), lambda: self.column(low + 2), lambda: self.at.dev(1))
        else:
            self.send(7, lambda: self.two(6, False), lambda: self.two(7, False), lambda: self.at.dev(1))
        self.got(7 + d, self.column(high))
        if d < 3:
            self.send(8 + d, lambda: self.column(high), lambda: self.column(high + 2), lambda: self.at.dev(-1))
        else:
            self.send(11, lambda: self.two(5, True), lambda: self.two(7, True), lambda: self.at.dev(-1))
        self.over(d)

    def w(self):
        for d in range(5):
            self.got(12 + d, self.columns(d, True))


def attend(kv, q_ref, s_scr, acc, peak, zs, h):
    tiles, width = 4, 256
    where = [(y, c) for y in range(NY) for c in range(NC)]

    def scores(j):
        top = None
        for a, (y, c) in enumerate(where):
            t = jnp.dot(
                kv[zs, y, c, 0:256, :],
                q_ref[h, :, j * width : (j + 1) * width],
                preferred_element_type=jnp.float32,
            )
            s_scr[j % 2, a * 256 : (a + 1) * 256, :] = t
            t = jnp.max(t.reshape(32, 8, width), axis=0)
            top = t if top is None else jnp.maximum(top, t)
        return top

    ones = jnp.ones((16, 256), jnp.bfloat16)
    later = scores(0)
    for j in range(tiles):
        top = later
        if j + 1 < tiles:
            later = scores(j + 1)
        cols = slice(j * width, (j + 1) * width)
        before = peak[h, 0:1, cols]
        now = jnp.maximum(before, jnp.max(top, axis=0, keepdims=True) * SCALE)
        peak[h, 0:1, cols] = now
        rescale = jnp.exp2(before - now)
        added = None
        for a, (y, c) in enumerate(where):
            exps = jnp.exp2(s_scr[j % 2, a * 256 : (a + 1) * 256, :] * SCALE - now)
            first = kv[zs, y, c, pl.ds(pl.multiple_of(256 + h * HD, HD), HD), :]
            second = kv[zs, y, c, pl.ds(pl.multiple_of(384 + h * HD, HD), HD), :]
            left = jnp.concatenate([jnp.concatenate([first, second], axis=1), ones], axis=0)
            term = jnp.dot(left, exps.astype(jnp.bfloat16), preferred_element_type=jnp.float32)
            added = term if added is None else added + term
        acc[h, :, cols] = acc[h, :, cols] * rescale + added


def layer_kernel(
    q_ref, kv_in, up_in, down_in, ow_in, stream, gain, o_ref,
    kv, up, down, ow, s_scr, acc, peak, st, heads, mid, nrm, hid, part, arrived, transit, joined,
    kv_s, kv_r, up_s, up_r, down_s, down_r, ow_s, ow_r, tp_s, tp_r, own_sem,
):
    at = Place()
    own = [
        pltpu.make_async_copy(src, dst, own_sem.at[k])
        for k, (src, dst) in enumerate(
            (
                (kv_in, kv.at[0, at.y, at.core]),
                (up_in, up.at[0, at.y, at.core]),
                (down_in, down.at[0, at.y, at.core]),
                (ow_in, ow.at[0]),
                (stream.at[at.x], st),
            )
        )
    ]
    for copy in own:
        copy.start()
    barrier = pltpu.get_barrier_semaphore()
    nearby = [at.dev(1), at.dev(-1), at.dev(0, 1), at.dev(0, -1), at.other()]
    nearby += [at.along(1), at.along(-1), at.along(2)]
    for near in nearby:
        pl.semaphore_signal(barrier, inc=1, device_id=near, device_id_type=MESH)
    acc[...] = jnp.zeros_like(acc)
    peak[...] = jnp.full_like(peak, -1e30)
    pl.semaphore_wait(barrier, len(nearby))
    pairs = ZFirst(kv_in, kv, 256, at, kv_s, kv_r)
    ups = YFirst(up_in, up, 16, at, up_s, up_r)
    downs = ZFirst(down_in, down, 16, at, down_s, down_r)
    outs = Around(ow_in, ow, 128, at, ow_s, ow_r)
    across = Mail(at, tp_s, tp_r)

    pairs.a(0)
    ups.s1()
    outs.s1()
    pairs.a(1)
    pairs.b(0)
    ups.s2()
    pairs.b(1)
    pairs.a(2)
    own[0].wait()
    pairs.c(0)
    downs.a(0)
    own[1].wait()
    ups.s3()
    pairs.w(0)
    polls = {
        1: (lambda: pairs.c(1),),
        2: (lambda: pairs.w(1),),
        3: (lambda: pairs.b(2), lambda: pairs.a(3), lambda: downs.a(1),),
        4: (outs.s2,),
        5: (lambda: pairs.c(2),),
        6: (lambda: pairs.w(2), lambda: ups.z(1),),
        7: (lambda: pairs.b(3),),
        8: (lambda: pairs.a(4), lambda: downs.b(0), lambda: downs.a(2),),
        9: (lambda: pairs.c(3), outs.s3,),
        10: (lambda: pairs.b(4), lambda: downs.b(1), lambda: ups.z(2), lambda: pairs.w(3),),
        13: (lambda: downs.a(3), lambda: pairs.c(4),),
        14: (lambda: pairs.w(4),),
        15: (lambda: downs.b(2), lambda: ups.z(3),),
    }

    def step(n, carry):
        def poll(keys):
            if len(keys) == 1:

                @pl.when(n == keys[0])
                def _():
                    for do in polls[keys[0]]:
                        do()

            else:
                at_half = len(keys) // 2
                pl.when(n < keys[at_half])(lambda: poll(keys[:at_half]))
                pl.when(n >= keys[at_half])(lambda: poll(keys[at_half:]))

        poll(sorted(polls))
        attend(kv, q_ref, s_scr, acc, peak, n // 2, lax.rem(n, 2))
        return carry

    lax.fori_loop(0, 2 * NZ, step, 0)

    for k in range(4):
        sides = []
        for g in (2 * k, 2 * k + 1):
            h, cols = g // 4, slice(g % 4 * 256, (g % 4 + 1) * 256)
            sides.append(jnp.transpose(acc[h, 0:HD, cols] / acc[h, HD : HD + 1, cols]))
        both = jnp.concatenate(sides, axis=1).astype(jnp.bfloat16)
        heads[0, :, :, k * 128 : (k + 1) * 128] = both.reshape(NX, 64, 128)
    offsets = (0, -1, 1, 2)
    own[3].wait()
    own[4].wait()
    outs.w()
    across.send(2, lambda: heads.at[0, at.xat(2)], lambda: heads.at[1, 2], lambda: at.along(2))
    across.send(0, lambda: heads.at[0, at.xat(1)], lambda: heads.at[1, 0], lambda: at.along(1))
    across.send(1, lambda: heads.at[0, at.xat(-1)], lambda: heads.at[1, 1], lambda: at.along(-1))
    own[2].wait()
    downs.c(0)
    downs.a(4)
    downs.b(3)
    downs.c(1)
    for k in range(3):
        across.got(k, heads.at[1, k])
    lefts = [heads[0, at.x], heads[1, 0], heads[1, 1], heads[1, 2]]
    for j in range(5):
        if j < 4:
            cols = slice(j * 512, (j + 1) * 512)
            attended = None
            for i, left in enumerate(lefts):
                term = jnp.dot(left[:, 0:256], ow[i, 0, :, cols], preferred_element_type=jnp.float32)
                term += jnp.dot(left[:, 256:512], ow[i, 1, :, cols], preferred_element_type=jnp.float32)
                term = term.astype(jnp.bfloat16).astype(jnp.float32)
                attended = term if attended is None else attended + term
            mid[at.x, j] = (st[:, cols].astype(jnp.float32) + attended).astype(jnp.bfloat16)
        if j > 0:
            chunk = lambda j=j: mid.at[at.x, j - 1]
            across.send(3 + j - 1, chunk, chunk, lambda: at.along(1))
            across.send(7 + j - 1, chunk, chunk, lambda: at.along(-1))

    def norm(i):
        rows = jnp.concatenate([mid[at.xat(offsets[i]), j] for j in range(4)], axis=1)
        rows = rows.astype(jnp.float32)
        mean = jnp.mean(rows * rows, axis=-1, keepdims=True)
        nrm[i * 64 : (i + 1) * 64, :] = (rows * lax.rsqrt(mean + EPSILON) * gain[...]).astype(jnp.bfloat16)

    def slot_z(k):
        return at.z if k == 0 else lax.rem(at.z + (4 if k == 7 else (k + 1) // 2 if k % 2 else NZ - k // 2), NZ)

    def lift(first, last):
        rows = slice(first * 64, last * 64)
        for t in range(4):
            cols = slice(t * 512, (t + 1) * 512)
            sums = None
            for k in range(NZ):
                left = nrm[rows, pl.ds(pl.multiple_of(slot_z(k) * 256, 256), 256)]
                term = jnp.dot(left, up[k, :, :, :, cols].reshape(256, 512), preferred_element_type=jnp.float32)
                sums = term if sums is None else sums + term
            hid[rows, cols] = jnp.square(jnp.maximum(sums, 0.0)).astype(jnp.bfloat16)

    norm(0)
    for j in (0, 1):
        chunk = lambda j=j: mid.at[at.xat(-1), j]
        across.got(3 + j, chunk())
        across.send(11 + j, chunk, chunk, lambda: at.along(1))
    for j in (2, 3):
        chunk = lambda j=j: mid.at[at.xat(1), j]
        across.got(7 + j, chunk())
        across.send(11 + j, chunk, chunk, lambda: at.along(-1))
    downs.b(4)
    ups.z(4)
    downs.c(2)
    ups.w()
    downs.w(1)
    downs.w(0)
    downs.c(4)
    downs.c(3)
    lift(0, 1)
    for j in (2, 3):
        across.got(3 + j, mid.at[at.xat(-1), j])
    for j in (0, 1):
        across.got(7 + j, mid.at[at.xat(1), j])
    norm(1)
    norm(2)
    lift(1, 3)
    for j in range(4):
        across.got(11 + j, mid.at[at.xat(2), j])
    norm(3)
    lift(3, 4)
    downs.w(3)
    downs.w(2)
    downs.w(4)

    def lower(k):
        for t in range(2):
            r = lax.rem(2 * at.xat(k) + t + NZ - at.z, NZ)
            where = jnp.where(r > 4, 2 * (NZ - r), jnp.maximum(2 * r - 1, 0))
            sums = lax.dot_general(
                hid[...],
                down[where].reshape(256, 2048),
                (((1,), (1,)), ((), ())),
                preferred_element_type=jnp.float32,
            ).astype(jnp.bfloat16)
            for i in range(4):
                part[k, at.xat(offsets[i]), :, t * 256 : (t + 1) * 256] = sums[i * 64 : (i + 1) * 64]

    lower(2)
    lower(1)
    first, second = pl.ds(0, 2), pl.ds(2, 2)
    across.send(15, lambda: part.at[2, first], lambda: transit.at[0], lambda: at.along(1))
    across.send(16, lambda: part.at[2, second], lambda: transit.at[1], lambda: at.along(-1))
    lower(3)
    across.send(17, lambda: part.at[1, second], lambda: arrived.at[0, second], lambda: at.along(1))
    lower(0)
    across.send(18, lambda: part.at[3, first], lambda: arrived.at[1, first], lambda: at.along(-1))
    across.got(15, transit.at[0])
    for s in range(2):
        total = part[1, s].astype(jnp.float32) + transit[0, s].astype(jnp.float32)
        joined[0, s] = total.astype(jnp.bfloat16)
    across.got(16, transit.at[1])
    for s in range(2):
        total = part[3, 2 + s].astype(jnp.float32) + transit[1, s].astype(jnp.float32)
        joined[1, s] = total.astype(jnp.bfloat16)
    across.send(19, lambda: joined.at[0], lambda: arrived.at[0, first], lambda: at.along(1))
    across.send(20, lambda: joined.at[1], lambda: arrived.at[1, second], lambda: at.along(-1))
    across.got(17, arrived.at[0, second])
    across.got(18, arrived.at[1, first])
    across.got(19, arrived.at[0, first])
    across.got(20, arrived.at[1, second])
    for s in range(NX):
        total = mid[s, at.x].astype(jnp.float32) + part[0, s].astype(jnp.float32)
        for k in range(2):
            total += arrived[k, s].astype(jnp.float32)
        o_ref[s] = total.astype(jnp.bfloat16)
    for mail in (pairs, ups, downs, outs, across):
        mail.finish()


def layer(*operands):
    anywhere = pl.BlockSpec(memory_space=pl.ANY)
    vmem = pl.BlockSpec(memory_space=pltpu.VMEM)
    bf16, f32 = jnp.bfloat16, jnp.float32
    held = [
        ((NZ, NY, NC, 512, 128), bf16),
        ((NZ, NY, NC, 32, 2048), bf16),
        ((NZ, NY, NC, 32, 2048), bf16),
        ((NX, 2, 256, 2048), bf16),
        ((2, 2048, 256), f32),
        ((2, 80, 1024), f32),
        ((2, 8, 1024), f32),
        ((64, 2048), bf16),
        ((2, NX, 64, 512), bf16),
        ((NX, 4, 64, 512), bf16),
        ((256, 2048), bf16),
        ((256, 2048), bf16),
        ((NX, NX, 64, 512), bf16),
        ((2, NX, 64, 512), bf16),
        ((2, 2, 64, 512), bf16),
        ((2, 2, 64, 512), bf16),
    ]
    counts = (33, 33, 17, 17, 33, 33, 7, 7, 21, 21, 5)
    return pl.pallas_call(
        layer_kernel,
        name="layer",
        out_shape=jax.ShapeDtypeStruct((NX, 64, 512), bf16),
        in_specs=[vmem, anywhere, anywhere, anywhere, anywhere, anywhere, vmem],
        out_specs=vmem,
        scratch_shapes=[
            *(pltpu.VMEM(shape, kind) for shape, kind in held),
            *(pltpu.SemaphoreType.DMA((n,)) for n in counts),
        ],
        compiler_params=pltpu.CompilerParams(
            collective_id=0, has_side_effects=True, vmem_limit_bytes=60 * 1024 * 1024
        ),
    )(*operands)


def shards(
    queries,
    keys,
    values,
    query_gain,
    key_gain,
    stream,
    out_weight,
    mixer_gain,
    up_weight,
    down_weight,
):
    rows = queries.shape[0]
    offset = lax.axis_index("sp") * rows
    pq = prepare(queries, query_gain, offset)
    pq = jnp.transpose(pq.reshape(rows, 2, 4, HD), (1, 3, 2, 0)).reshape(2, HD, 4 * rows)
    none = jnp.zeros((1, HD, 4 * rows), jnp.bfloat16)
    q_wide = jnp.concatenate(
        [jnp.concatenate([pq[:1], none], axis=1), jnp.concatenate([none, pq[1:]], axis=1)], axis=0
    )
    pk = prepare(keys, key_gain, offset).reshape(rows, 128)
    v_turned = jnp.transpose(values.reshape(2, 128, 128), (0, 2, 1)).reshape(256, 128)
    kv_block = jnp.concatenate([pk, v_turned], axis=0)
    out_block = out_weight.reshape(2, 256, -1)
    width = stream.shape[1]
    updated = layer(
        q_wide,
        kv_block,
        up_weight,
        down_weight.T,
        out_block,
        stream.reshape(NX, rows // NX, width),
        mixer_gain.reshape(1, width),
    )
    return updated.reshape(rows, -1)


def solution(mesh):
    return jax.shard_map(
        shards,
        mesh=mesh,
        in_specs=(
            P("sp", "tp"),
            P("sp", "tp"),
            P("sp", "tp"),
            P(),
            P(),
            P("sp", None),
            P("tp", None),
            P(),
            P("sp", "tp"),
            P("tp", "sp"),
        ),
        out_specs=P("sp", "tp"),
        check_vma=False,
    )
```

```python
import math

import jax
import jax.numpy as jnp
from jax import lax
from jax.experimental import pallas as pl
from jax.experimental.pallas import tpu as pltpu
from jax.sharding import PartitionSpec as P

HD = 64
GRID_W = 64
EPSILON = 1e-06
NX, NZ, NY, NC = 4, 8, 4, 2
SCALE = math.log2(math.e) / math.sqrt(HD)
MESH = pl.DeviceIdType.MESH


def prepare(projected, gains, offset):
    row_count = projected.shape[0]
    head_count = projected.shape[1] // HD
    widened = projected.astype(jnp.float32).reshape(row_count, head_count, HD)
    widened = (
        widened
        * lax.rsqrt(jnp.mean(widened * widened, axis=-1, keepdims=True) + EPSILON)
        * gains
    )
    position = offset + jnp.arange(row_count, dtype=jnp.int32)
    grid_row = (position // GRID_W).astype(jnp.float32)
    grid_col = (position % GRID_W).astype(jnp.float32)
    half_dim = HD // 2
    inverse = 1.0 / jnp.power(10000.0, jnp.arange(0, half_dim, 2, dtype=jnp.float32) / half_dim)
    angle = jnp.concatenate([grid_row[:, None] * inverse, grid_col[:, None] * inverse], axis=-1)
    cosine = jnp.cos(angle)[:, None, :]
    sine_table = jnp.sin(angle)[:, None, :]
    paired = widened.reshape(row_count, head_count, half_dim, 2)
    former = paired[..., 0]
    latter = paired[..., 1]
    rotated = jnp.stack(
        [former * cosine - latter * sine_table, former * sine_table + latter * cosine], axis=-1
    )
    return rotated.reshape(row_count, head_count, HD).astype(jnp.bfloat16)


class Place:
    def __init__(self):
        me = lax.axis_index("sp")
        self.core = lax.rem(me, NC)
        self.y = lax.rem(me // NC, NY)
        self.z = me // (NC * NY)
        self.x = lax.axis_index("tp")

    def yat(self, d):
        return lax.rem(self.y + (d + NY) % NY, NY)

    def xat(self, d):
        return lax.rem(self.x + (d + NX) % NX, NX)

    def dev(self, dz=0, dy=0):
        return {"sp": (lax.rem(self.z + (dz + NZ) % NZ, NZ) * NY + self.yat(dy)) * NC + self.core}

    def other(self):
        return {"sp": (self.z * NY + self.y) * NC + 1 - self.core}

    def along(self, dx):
        return {"tp": self.xat(dx)}


class Mail:
    def __init__(self, place, send_sems, recv_sems):
        self.at, self.ss, self.rs, self.sent = place, send_sems, recv_sems, []

    def copy(self, key, src, dst, target):
        return pltpu.make_async_remote_copy(
            src_ref=src,
            dst_ref=dst,
            send_sem=self.ss.at[key],
            recv_sem=self.rs.at[key],
            device_id=target,
            device_id_type=MESH,
        )

    def send(self, key, src, dst, target):
        self.copy(key, src(), dst(), target()).start()
        self.sent.append((key, src, dst, target))

    def got(self, key, ref):
        self.copy(key, ref, ref, self.at.other()).wait_recv()

    def finish(self):
        for key, src, dst, target in self.sent:
            self.copy(key, src(), dst(), target()).wait_send()


class Around(Mail):
    SEMS = 7

    def __init__(self, own, buf, half, *rest):
        super().__init__(*rest)
        self.own, self.buf, self.half = own, buf, half

    def slot(self, k):
        return self.buf.at[k, self.at.core]

    def part(self, k, second):
        return self.buf.at[k, self.at.core, pl.ds(self.half if second else 0, self.half)]

    def over(self, k):
        self.send(3 + k, lambda: self.slot(k), lambda: self.slot(k), self.at.other)

    def s1(self):
        own = lambda: self.own.at[self.at.core]
        self.send(0, own, lambda: self.slot(1), lambda: self.at.along(1))
        self.send(1, own, lambda: self.slot(2), lambda: self.at.along(-1))

    def s2(self):
        self.got(0, self.slot(1))
        self.send(2, lambda: self.part(1, False), lambda: self.part(3, False), lambda: self.at.along(1))
        self.got(1, self.slot(2))
        self.send(3, lambda: self.part(2, True), lambda: self.part(3, True), lambda: self.at.along(-1))
        self.over(1)
        self.over(2)

    def s3(self):
        self.got(2, self.part(3, False))
        self.got(3, self.part(3, True))
        self.over(3)

    def w(self):
        for k in (1, 2, 3):
            self.got(3 + k, self.buf.at[k, 1 - self.at.core])


class ZFirst(Mail):
    SEMS = 33

    def __init__(self, own, buf, half, *rest):
        super().__init__(*rest)
        self.own, self.buf, self.half = own, buf, half

    def slot(self, k):
        return self.buf.at[k, self.at.y, self.at.core]

    def part(self, k, dy, second):
        return self.buf.at[k, self.at.yat(dy), self.at.core, pl.ds(self.half if second else 0, self.half)]

    def slots(self, d):
        return pl.ds(0, 1) if d == 0 else pl.ds(7, 1) if d == 4 else pl.ds(2 * d - 1, 2)

    def pair(self, d, dy=0):
        return self.buf.at[self.slots(d), self.at.yat(dy), self.at.core]

    def columns(self, d, other=False):
        core = 1 - self.at.core if other else self.at.core
        return self.buf.at[self.slots(d), :, core]

    def along_y(self, d):
        self.send(8 + d, lambda: self.pair(d), lambda: self.pair(d), lambda: self.at.dev(0, 1))
        self.send(13 + d, lambda: self.pair(d), lambda: self.pair(d), lambda: self.at.dev(0, -1))

    def a(self, d):
        if d == 0:
            self.send(8, lambda: self.own, lambda: self.slot(0), lambda: self.at.dev(0, 1))
            self.send(13, lambda: self.own, lambda: self.slot(0), lambda: self.at.dev(0, -1))
            self.send(0, lambda: self.own, lambda: self.slot(2), lambda: self.at.dev(1))
            self.send(4, lambda: self.own, lambda: self.slot(1), lambda: self.at.dev(-1))
            return
        if d == 4:
            self.got(3, self.part(7, 0, False))
            self.got(7, self.part(7, 0, True))
        else:
            low, high = 2 * d, 2 * d - 1
            self.got(d - 1, self.slot(low))
            if d < 3:
                self.send(d, lambda: self.slot(low), lambda: self.slot(low + 2), lambda: self.at.dev(1))
            else:
                self.send(3, lambda: self.part(6, 0, False), lambda: self.part(7, 0, False), lambda: self.at.dev(1))
            self.got(3 + d, self.slot(high))
            if d < 3:
                self.send(4 + d, lambda: self.slot(high), lambda: self.slot(high + 2), lambda: self.at.dev(-1))
            else:
                self.send(7, lambda: self.part(5, 0, True), lambda: self.part(7, 0, True), lambda: self.at.dev(-1))
        self.along_y(d)

    def piece(self, d, dy, second):
        if d in (0, 4):
            return self.part(0 if d == 0 else 7, dy, second)
        return self.buf.at[2 * d if second else 2 * d - 1, self.at.yat(dy), self.at.core]

    def b(self, d):
        self.got(8 + d, self.pair(d, -1))
        one = lambda: self.piece(d, -1, False)
        self.send(18 + d, one, one, lambda: self.at.dev(0, 1))
        self.got(13 + d, self.pair(d, 1))
        two = lambda: self.piece(d, 1, True)
        self.send(23 + d, two, two, lambda: self.at.dev(0, -1))

    def c(self, d):
        self.got(18 + d, self.piece(d, 2, False))
        self.got(23 + d, self.piece(d, 2, True))
        self.send(28 + d, lambda: self.columns(d), lambda: self.columns(d), self.at.other)

    def w(self, d):
        self.got(28 + d, self.columns(d, True))


class YFirst(Mail):
    SEMS = 17

    def __init__(self, own, buf, half, *rest):
        super().__init__(*rest)
        self.own, self.buf, self.half = own, buf, half

    def slot(self, dy):
        return self.buf.at[0, self.at.yat(dy), self.at.core]

    def part(self, dy, second):
        return self.slot(dy).at[pl.ds(self.half if second else 0, self.half)]

    def column(self, k):
        return self.buf.at[k, :, self.at.core]

    def two(self, k, second):
        return self.buf.at[k, pl.ds(2 if second else 0, 2), self.at.core]

    def columns(self, d, other=False):
        core = 1 - self.at.core if other else self.at.core
        return self.buf.at[pl.ds(0, 1) if d == 0 else pl.ds(7, 1) if d == 4 else pl.ds(2 * d - 1, 2), :, core]

    def over(self, d):
        self.send(12 + d, lambda: self.columns(d), lambda: self.columns(d), self.at.other)

    def s1(self):
        self.send(0, lambda: self.own, lambda: self.slot(0), lambda: self.at.dev(0, 1))
        self.send(1, lambda: self.own, lambda: self.slot(0), lambda: self.at.dev(0, -1))

    def s2(self):
        self.got(0, self.slot(-1))
        one = lambda: self.part(-1, False)
        self.send(2, one, one, lambda: self.at.dev(0, 1))
        self.got(1, self.slot(1))
        two = lambda: self.part(1, True)
        self.send(3, two, two, lambda: self.at.dev(0, -1))

    def s3(self):
        self.got(2, self.part(2, False))
        self.got(3, self.part(2, True))
        self.send(4, lambda: self.column(0), lambda: self.column(2), lambda: self.at.dev(1))
        self.send(8, lambda: self.column(0), lambda: self.column(1), lambda: self.at.dev(-1))
        self.over(0)

    def z(self, d):
        if d == 4:
            self.got(7, self.two(7, False))
            self.got(11, self.two(7, True))
            self.over(4)
            return
        low, high = 2 * d, 2 * d - 1
        self.got(3 + d, self.column(low))
        if d < 3:
            self.send(4 + d, lambda: self.column(low), lambda: self.column(low + 2), lambda: self.at.dev(1))
        else:
            self.send(7, lambda: self.two(6, False), lambda: self.two(7, False), lambda: self.at.dev(1))
        self.got(7 + d, self.column(high))
        if d < 3:
            self.send(8 + d, lambda: self.column(high), lambda: self.column(high + 2), lambda: self.at.dev(-1))
        else:
            self.send(11, lambda: self.two(5, True), lambda: self.two(7, True), lambda: self.at.dev(-1))
        self.over(d)

    def w(self):
        for d in range(5):
            self.got(12 + d, self.columns(d, True))


def attend(kv, q_ref, s_scr, acc, peak, zs, h):
    tiles, width = 4, 256
    where = [(y, c) for y in range(NY) for c in range(NC)]

    def scores(j):
        top = None
        for a, (y, c) in enumerate(where):
            t = jnp.dot(
                kv[zs, y, c, 0:256, :],
                q_ref[h, :, j * width : (j + 1) * width],
                preferred_element_type=jnp.float32,
            )
            s_scr[j % 2, a * 256 : (a + 1) * 256, :] = t
            t = jnp.max(t.reshape(32, 8, width), axis=0)
            top = t if top is None else jnp.maximum(top, t)
        return top

    ones = jnp.ones((16, 256), jnp.bfloat16)
    later = scores(0)
    for j in range(tiles):
        top = later
        if j + 1 < tiles:
            later = scores(j + 1)
        cols = slice(j * width, (j + 1) * width)
        before = peak[h, 0:1, cols]
        now = jnp.maximum(before, jnp.max(top, axis=0, keepdims=True) * SCALE)
        peak[h, 0:1, cols] = now
        rescale = jnp.exp2(before - now)
        added = None
        for a, (y, c) in enumerate(where):
            exps = jnp.exp2(s_scr[j % 2, a * 256 : (a + 1) * 256, :] * SCALE - now)
            first = kv[zs, y, c, pl.ds(pl.multiple_of(256 + h * HD, HD), HD), :]
            second = kv[zs, y, c, pl.ds(pl.multiple_of(384 + h * HD, HD), HD), :]
            left = jnp.concatenate([jnp.concatenate([first, second], axis=1), ones], axis=0)
            term = jnp.dot(left, exps.astype(jnp.bfloat16), preferred_element_type=jnp.float32)
            added = term if added is None else added + term
        acc[h, :, cols] = acc[h, :, cols] * rescale + added


def layer_kernel(
    q_ref, kv_in, up_in, down_in, ow_in, stream, gain, o_ref,
    kv, up, down, ow, s_scr, acc, peak, st, heads, mid, nrm, hid, part, arrived, transit, joined,
    kv_s, kv_r, up_s, up_r, down_s, down_r, ow_s, ow_r, tp_s, tp_r, own_sem,
):
    at = Place()
    own = [
        pltpu.make_async_copy(src, dst, own_sem.at[k])
        for k, (src, dst) in enumerate(
            (
                (kv_in, kv.at[0, at.y, at.core]),
                (up_in, up.at[0, at.y, at.core]),
                (down_in, down.at[0, at.y, at.core]),
                (ow_in, ow.at[0]),
                (stream.at[at.x], st),
            )
        )
    ]
    for copy in own:
        copy.start()
    barrier = pltpu.get_barrier_semaphore()
    nearby = [at.dev(1), at.dev(-1), at.dev(0, 1), at.dev(0, -1), at.other()]
    nearby += [at.along(1), at.along(-1), at.along(2)]
    for near in nearby:
        pl.semaphore_signal(barrier, inc=1, device_id=near, device_id_type=MESH)
    acc[...] = jnp.zeros_like(acc)
    peak[...] = jnp.full_like(peak, -1e30)
    pl.semaphore_wait(barrier, len(nearby))
    pairs = ZFirst(kv_in, kv, 256, at, kv_s, kv_r)
    ups = YFirst(up_in, up, 16, at, up_s, up_r)
    downs = ZFirst(down_in, down, 16, at, down_s, down_r)
    outs = Around(ow_in, ow, 128, at, ow_s, ow_r)
    across = Mail(at, tp_s, tp_r)

    ups.s1()
    outs.s1()
    pairs.a(0)
    pairs.a(1)
    pairs.b(0)
    ups.s2()
    pairs.b(1)
    pairs.a(2)
    own[0].wait()
    pairs.c(0)
    pairs.w(0)
    pairs.a(3)
    pairs.c(1)
    own[1].wait()
    ups.s3()
    polls = {
        1: (lambda: pairs.w(1),),
        2: (lambda: pairs.b(2),),
        4: (lambda: pairs.a(4), lambda: pairs.b(3), lambda: downs.a(0), outs.s2,),
        5: (lambda: pairs.c(2),),
        6: (lambda: downs.a(1), lambda: pairs.b(4), lambda: ups.z(1), lambda: pairs.w(2),),
        8: (lambda: pairs.c(3),),
        9: (outs.s3,),
        10: (lambda: downs.a(2), lambda: pairs.w(3),),
        12: (lambda: ups.z(2), lambda: pairs.c(4),),
        13: (lambda: downs.a(3),),
        14: (lambda: pairs.w(4),),
        15: (lambda: downs.b(2),),
    }

    def step(n, carry):
        def poll(keys):
            if len(keys) == 1:

                @pl.when(n == keys[0])
                def _():
                    for do in polls[keys[0]]:
                        do()

            else:
                at_half = len(keys) // 2
                pl.when(n < keys[at_half])(lambda: poll(keys[:at_half]))
                pl.when(n >= keys[at_half])(lambda: poll(keys[at_half:]))

        poll(sorted(polls))
        attend(kv, q_ref, s_scr, acc, peak, n // 2, lax.rem(n, 2))
        return carry

    lax.fori_loop(0, 2 * NZ, step, 0)

    for k in range(4):
        sides = []
        for g in (2 * k, 2 * k + 1):
            h, cols = g // 4, slice(g % 4 * 256, (g % 4 + 1) * 256)
            sides.append(jnp.transpose(acc[h, 0:HD, cols] / acc[h, HD : HD + 1, cols]))
        both = jnp.concatenate(sides, axis=1).astype(jnp.bfloat16)
        heads[0, :, :, k * 128 : (k + 1) * 128] = both.reshape(NX, 64, 128)
    offsets = (0, -1, 1, 2)
    own[3].wait()
    own[4].wait()
    across.send(2, lambda: heads.at[0, at.xat(2)], lambda: heads.at[1, 2], lambda: at.along(2))
    across.send(0, lambda: heads.at[0, at.xat(1)], lambda: heads.at[1, 0], lambda: at.along(1))
    across.send(1, lambda: heads.at[0, at.xat(-1)], lambda: heads.at[1, 1], lambda: at.along(-1))
    outs.w()
    downs.b(0)
    downs.b(1)
    downs.c(2)
    ups.z(3)
    downs.a(4)
    for k in range(3):
        across.got(k, heads.at[1, k])
    lefts = [heads[0, at.x], heads[1, 0], heads[1, 1], heads[1, 2]]
    for j in range(5):
        if j < 4:
            cols = slice(j * 512, (j + 1) * 512)
            attended = None
            for i, left in enumerate(lefts):
                term = jnp.dot(left[:, 0:256], ow[i, 0, :, cols], preferred_element_type=jnp.float32)
                term += jnp.dot(left[:, 256:512], ow[i, 1, :, cols], preferred_element_type=jnp.float32)
                term = term.astype(jnp.bfloat16).astype(jnp.float32)
                attended = term if attended is None else attended + term
            mid[at.x, j] = (st[:, cols].astype(jnp.float32) + attended).astype(jnp.bfloat16)
        if j > 0:
            chunk = lambda j=j: mid.at[at.x, j - 1]
            across.send(3 + j - 1, chunk, chunk, lambda: at.along(1))
            across.send(7 + j - 1, chunk, chunk, lambda: at.along(-1))

    def norm(i):
        rows = jnp.concatenate([mid[at.xat(offsets[i]), j] for j in range(4)], axis=1)
        rows = rows.astype(jnp.float32)
        mean = jnp.mean(rows * rows, axis=-1, keepdims=True)
        nrm[i * 64 : (i + 1) * 64, :] = (rows * lax.rsqrt(mean + EPSILON) * gain[...]).astype(jnp.bfloat16)

    def slot_z(k):
        return at.z if k == 0 else lax.rem(at.z + (4 if k == 7 else (k + 1) // 2 if k % 2 else NZ - k // 2), NZ)

    def lift(first, last):
        rows = slice(first * 64, last * 64)
        for t in range(4):
            cols = slice(t * 512, (t + 1) * 512)
            sums = None
            for k in range(NZ):
                left = nrm[rows, pl.ds(pl.multiple_of(slot_z(k) * 256, 256), 256)]
                term = jnp.dot(left, up[k, :, :, :, cols].reshape(256, 512), preferred_element_type=jnp.float32)
                sums = term if sums is None else sums + term
            hid[rows, cols] = jnp.square(jnp.maximum(sums, 0.0)).astype(jnp.bfloat16)

    downs.b(3)
    ups.z(4)
    norm(0)
    for j in (0, 1):
        chunk = lambda j=j: mid.at[at.xat(-1), j]
        across.got(3 + j, chunk())
        across.send(11 + j, chunk, chunk, lambda: at.along(1))
    for j in (2, 3):
        chunk = lambda j=j: mid.at[at.xat(1), j]
        across.got(7 + j, chunk())
        across.send(11 + j, chunk, chunk, lambda: at.along(-1))
    for j in (2, 3):
        across.got(3 + j, mid.at[at.xat(-1), j])
    for j in (0, 1):
        across.got(7 + j, mid.at[at.xat(1), j])
    norm(1)
    norm(2)
    downs.c(1)
    own[2].wait()
    downs.c(0)
    downs.b(4)
    ups.w()
    lift(0, 3)
    downs.c(4)
    downs.c(3)
    for j in range(4):
        across.got(11 + j, mid.at[at.xat(2), j])
    norm(3)
    lift(3, 4)
    downs.w(0)
    downs.w(1)
    downs.w(4)
    downs.w(2)
    downs.w(3)

    def lower(k):
        for t in range(2):
            r = lax.rem(2 * at.xat(k) + t + NZ - at.z, NZ)
            where = jnp.where(r > 4, 2 * (NZ - r), jnp.maximum(2 * r - 1, 0))
            sums = lax.dot_general(
                hid[...],
                down[where].reshape(256, 2048),
                (((1,), (1,)), ((), ())),
                preferred_element_type=jnp.float32,
            ).astype(jnp.bfloat16)
            for i in range(4):
                part[k, at.xat(offsets[i]), :, t * 256 : (t + 1) * 256] = sums[i * 64 : (i + 1) * 64]

    lower(2)
    lower(1)
    first, second = pl.ds(0, 2), pl.ds(2, 2)
    across.send(15, lambda: part.at[2, first], lambda: transit.at[0], lambda: at.along(1))
    across.send(16, lambda: part.at[2, second], lambda: transit.at[1], lambda: at.along(-1))
    lower(3)
    across.send(17, lambda: part.at[1, second], lambda: arrived.at[0, second], lambda: at.along(1))
    lower(0)
    across.send(18, lambda: part.at[3, first], lambda: arrived.at[1, first], lambda: at.along(-1))
    across.got(15, transit.at[0])
    for s in range(2):
        total = part[1, s].astype(jnp.float32) + transit[0, s].astype(jnp.float32)
        joined[0, s] = total.astype(jnp.bfloat16)
    across.got(16, transit.at[1])
    for s in range(2):
        total = part[3, 2 + s].astype(jnp.float32) + transit[1, s].astype(jnp.float32)
        joined[1, s] = total.astype(jnp.bfloat16)
    across.send(19, lambda: joined.at[0], lambda: arrived.at[0, first], lambda: at.along(1))
    across.send(20, lambda: joined.at[1], lambda: arrived.at[1, second], lambda: at.along(-1))
    across.got(17, arrived.at[0, second])
    across.got(18, arrived.at[1, first])
    across.got(19, arrived.at[0, first])
    across.got(20, arrived.at[1, second])
    for s in range(NX):
        total = mid[s, at.x].astype(jnp.float32) + part[0, s].astype(jnp.float32)
        for k in range(2):
            total += arrived[k, s].astype(jnp.float32)
        o_ref[s] = total.astype(jnp.bfloat16)
    for mail in (pairs, ups, downs, outs, across):
        mail.finish()


def layer(*operands):
    anywhere = pl.BlockSpec(memory_space=pl.ANY)
    vmem = pl.BlockSpec(memory_space=pltpu.VMEM)
    bf16, f32 = jnp.bfloat16, jnp.float32
    held = [
        ((NZ, NY, NC, 512, 128), bf16),
        ((NZ, NY, NC, 32, 2048), bf16),
        ((NZ, NY, NC, 32, 2048), bf16),
        ((NX, 2, 256, 2048), bf16),
        ((2, 2048, 256), f32),
        ((2, 80, 1024), f32),
        ((2, 8, 1024), f32),
        ((64, 2048), bf16),
        ((2, NX, 64, 512), bf16),
        ((NX, 4, 64, 512), bf16),
        ((256, 2048), bf16),
        ((256, 2048), bf16),
        ((NX, NX, 64, 512), bf16),
        ((2, NX, 64, 512), bf16),
        ((2, 2, 64, 512), bf16),
        ((2, 2, 64, 512), bf16),
    ]
    counts = (33, 33, 17, 17, 33, 33, 7, 7, 21, 21, 5)
    return pl.pallas_call(
        layer_kernel,
        name="layer",
        out_shape=jax.ShapeDtypeStruct((NX, 64, 512), bf16),
        in_specs=[vmem, anywhere, anywhere, anywhere, anywhere, anywhere, vmem],
        out_specs=vmem,
        scratch_shapes=[
            *(pltpu.VMEM(shape, kind) for shape, kind in held),
            *(pltpu.SemaphoreType.DMA((n,)) for n in counts),
        ],
        compiler_params=pltpu.CompilerParams(
            collective_id=0, has_side_effects=True, vmem_limit_bytes=60 * 1024 * 1024
        ),
    )(*operands)


def shards(
    queries,
    keys,
    values,
    query_gain,
    key_gain,
    stream,
    out_weight,
    mixer_gain,
    up_weight,
    down_weight,
):
    rows = queries.shape[0]
    offset = lax.axis_index("sp") * rows
    pq = prepare(queries, query_gain, offset)
    pq = jnp.transpose(pq.reshape(rows, 2, 4, HD), (1, 3, 2, 0)).reshape(2, HD, 4 * rows)
    none = jnp.zeros((1, HD, 4 * rows), jnp.bfloat16)
    q_wide = jnp.concatenate(
        [jnp.concatenate([pq[:1], none], axis=1), jnp.concatenate([none, pq[1:]], axis=1)], axis=0
    )
    pk = prepare(keys, key_gain, offset).reshape(rows, 128)
    v_turned = jnp.transpose(values.reshape(2, 128, 128), (0, 2, 1)).reshape(256, 128)
    kv_block = jnp.concatenate([pk, v_turned], axis=0)
    out_block = out_weight.reshape(2, 256, -1)
    width = stream.shape[1]
    updated = layer(
        q_wide,
        kv_block,
        up_weight,
        down_weight.T,
        out_block,
        stream.reshape(NX, rows // NX, width),
        mixer_gain.reshape(1, width),
    )
    return updated.reshape(rows, -1)


def solution(mesh):
    return jax.shard_map(
        shards,
        mesh=mesh,
        in_specs=(
            P("sp", "tp"),
            P("sp", "tp"),
            P("sp", "tp"),
            P(),
            P(),
            P("sp", None),
            P("tp", None),
            P(),
            P("sp", "tp"),
            P("tp", "sp"),
        ),
        out_specs=P("sp", "tp"),
        check_vma=False,
    )
```
